128 devices in a mesh: ep: 16 (over z, x), tp: 8 (over y, core).
Axes of the slice: x: 4, y: 4, z: 4, core: 2. Of those that a mesh axis runs over, the one named last changes fastest.
Arguments:
- query_latent: bfloat16 [16384, 768], P(('ep', 'tp')), may hold values from -6 to 6
- kv_latent: bfloat16 [16384, 512], P(('ep', 'tp')), may hold values from -6 to 6
- rope_key: bfloat16 [16384, 64], P(('ep', 'tp')), may hold values from -6 to 6
- query_gain: float32 [768], replicated, may hold values from 0.1 to 12
- kv_gain: float32 [512], replicated, may hold values from 0.1 to 12
- query_nope_w: bfloat16 [768, 1024], P(None, 'tp'), may hold values from -0.21875 to 0.21875
- query_rope_w: bfloat16 [768, 512], P(None, 'tp'), may hold values from -0.21875 to 0.21875
- key_up_w: bfloat16 [512, 1024], P(None, 'tp'), may hold values from -0.25 to 0.25
- value_up_w: bfloat16 [512, 1024], P(None, 'tp'), may hold values from -0.25 to 0.25
- output_w: bfloat16 [1024, 2048], P('tp'), may hold values from -0.1875 to 0.1875
- expert_in: bfloat16 [16384, 2048], P(('ep', 'tp')), may hold values from -6 to 6
- moe_gain: float32 [2048], replicated, may hold values from 0.1 to 12
- routes: int32 [16384, 2], P(('ep', 'tp')), may hold values from 0 to 31, all different within a row; in each aligned block of 128 rows (0 to 127, 128 to 255, ...) at most 10 rows name the same one
- route_weight: float32 [16384, 2], P(('ep', 'tp')), may hold values from 0.1 to 1
- gate_w: bfloat16 [32, 2048, 2048], P('ep', None, 'tp'), may hold values from -0.125 to 0.125
- up_w: bfloat16 [32, 2048, 2048], P('ep', None, 'tp'), may hold values from -0.125 to 0.125
- down_w: bfloat16 [32, 2048, 2048], P('ep', 'tp'), may hold values from -0.125 to 0.125
Outputs:
- mixer_out: bfloat16 [16384, 2048], P(('ep', 'tp'))
- expert_out: bfloat16 [16384, 2048], P(('ep', 'tp'))
The draws below stay inside these ranges and needn't reach their ends.
Inputs may be any that keep to these rules, and one draw needn't show every extreme that they name: `routes`: each row names 2 different experts; in the rows of one device no expert is named more than 10 times.
All inputs are finite; a program needn't handle non-finite values.
Results may differ from the reference program's by a relative error of at most 0.015.
The reference program's roundings to bfloat16 on the way count: a program that leaves them out, or rounds other values in their place, can miss the bound.
Values may be sent and summed in bfloat16 or wider, within the bound.
A program may use at most 128 MiB of HBM per device.

```python
import math
import jax
import jax.numpy as jnp
import numpy as np
from jax import lax

D = 2048
HEADS = 8
NOPE = 128
ROPE = 64
VDIM = 128
QLAT = 768
KVLAT = 512
FF = 2048
TOPK = 2
TOK_B = 128
EXPERTS = 32
CAP = 10
TOKENS_A = 16384
TOKENS_B = 16384
N_EP = 16
N_TP = 8


def gain_draw(key, count):
    return 1.0 + 0.18 * jnp.clip(jax.random.normal(key, (count,), jnp.float32), -5.0, 5.0)


def draw_query_gain(key, part):
    return gain_draw(jax.random.fold_in(key, 11), QLAT)


def draw_kv_gain(key, part):
    return gain_draw(jax.random.fold_in(key, 23), KVLAT)


def draw_moe_gain(key, part):
    return gain_draw(jax.random.fold_in(key, 37), D)


def levels(rng, dims, shards, low, top_value):
    loudness, own = 1.0, jax.random.fold_in(rng, 6)
    for position, blocks in shards:
        heights = jnp.exp(jax.random.uniform(jax.random.fold_in(own, position), (blocks,), jnp.float32, low / len(shards), top_value / len(shards)))
        loudness = loudness * jnp.repeat(heights, dims[position] // blocks).reshape([-1 if axis == position else 1 for axis in range(len(dims))])
    return loudness


def assign_block(own_key, own, number, rows, number_of, top, bound, skew):
    ranking = jax.random.permutation(own_key, number_of)
    packed, common = load_shares(number_of, rows * top, bound, skew, True), load_shares(number_of, rows * top, bound, skew, False)
    places = jnp.arange(number_of)

    def named(lengths, offset_by):
        used = int((lengths > 0).sum())
        fixed = max(1, used // 4)
        shifted = fixed + (places - fixed + offset_by * (used - fixed)) % max(1, number_of - fixed)
        return jnp.zeros((number_of,), jnp.int32).at[ranking[jnp.where(places < fixed, places, shifted)]].set(jnp.asarray(lengths, jnp.int32))

    lengths = jnp.where(number % 4 == 0, named(packed, number // 4), named(common, number - number // 4 - 1))
    mixed = jax.random.permutation(jax.random.fold_in(own, 3), number_of)
    donor, receiver = mixed[0:number_of // 2 * 2:2], mixed[1:number_of // 2 * 2:2]
    room = jnp.minimum(lengths[donor] - 1, bound - lengths[receiver]) // 2
    room = jnp.where((donor == ranking[0]) | (receiver == ranking[0]) | (lengths[receiver] == 0), 0, jnp.maximum(room, 0))
    shifted = jax.random.randint(jax.random.fold_in(own, 4), (number_of // 2,), 0, 1 << 20) % (room + 1)
    lengths = lengths.at[donor].add(-shifted).at[receiver].add(shifted)
    members = jnp.searchsorted(jnp.cumsum(lengths), jnp.arange(rows * top), side="right").astype(jnp.int32)
    listing = members.reshape(top, rows).T
    listing = listing[jax.random.permutation(jax.random.fold_in(own, 1), rows)]
    offset_by = jax.random.randint(jax.random.fold_in(own, 2), (rows, 1), 0, top)
    return jnp.take_along_axis(listing, (jnp.arange(top)[None, :] + offset_by) % top, axis=1)


def load_shares(count, total, bound, slope, full):
    weights = [(1 << 20) // math.isqrt(rank ** slope) + 1 for rank in range(1, count + 1)]
    largest = bound if full else min(bound, max(-(-total // count), total * weights[0] // sum(weights)))
    least = 1 if total - largest >= count - 1 else 0
    given, surplus = [largest] + [least] * (count - 1), total - largest - least * (count - 1)
    while surplus > 0:
        candidates = [i for i in range(1, count) if given[i] < largest] or [i for i in range(1, count) if given[i] < bound]
        pool, budget = sum([weights[i] for i in candidates]), surplus
        for i in candidates:
            extra = min(bound - given[i], max(1, budget * weights[i] // pool), surplus)
            given[i] = given[i] + extra
            surplus = surplus - extra
    return np.array(given)


def noise(stream_key, shape, scale, reach, shards=(), kind=jnp.bfloat16):
    entries = scale * jax.random.normal(stream_key, shape, jnp.float32)
    if shards:
        entries = entries * levels(stream_key, shape, shards, -0.22, 0.18)
    return jnp.clip(entries, -reach, reach).astype(kind)


def setup_inputs(seed: int = 0) -> dict:
    key_list = jax.random.split(jax.random.key(seed), 18)
    query_latent = noise(key_list[0], (TOKENS_A, QLAT), 1.0, 6.0, ((0, 128),))
    kv_latent = noise(key_list[1], (TOKENS_A, KVLAT), 1.0, 6.0, ((0, 128),))
    rope_key = noise(key_list[2], (TOKENS_A, ROPE), 1.0, 6.0, ((0, 128),))
    query_gain = draw_query_gain(jax.random.fold_in(key_list[17], 71), 0)
    kv_gain = draw_kv_gain(jax.random.fold_in(key_list[17], 71), 0)
    query_nope_w = noise(key_list[5], (QLAT, HEADS * NOPE), QLAT ** -0.5, 0.21875, ((1, 8),))
    query_rope_w = noise(key_list[6], (QLAT, HEADS * ROPE), QLAT ** -0.5, 0.21875, ((1, 8),))
    key_up_w = noise(key_list[7], (KVLAT, HEADS * NOPE), KVLAT ** -0.5, 0.25, ((1, 8),))
    value_up_w = noise(key_list[8], (KVLAT, HEADS * VDIM), KVLAT ** -0.5, 0.25, ((1, 8),))
    output_w = noise(key_list[9], (HEADS * VDIM, D), (HEADS * VDIM) ** -0.5, 0.1875, ((0, 8),))
    expert_in = noise(key_list[10], (TOKENS_B, D), 1.0, 6.0, ((0, 128),))
    moe_gain = draw_moe_gain(jax.random.fold_in(key_list[17], 71), 0)
    routes_keys = jax.random.split(jax.random.fold_in(key_list[12], 1), TOKENS_B // TOK_B)
    routes_turns = jax.random.permutation(jax.random.fold_in(key_list[12], 3), TOKENS_B // TOK_B)
    routes = jax.vmap(lambda own, number: assign_block(jax.random.fold_in(key_list[12], 2), own, number, TOK_B, EXPERTS, TOPK, CAP, 1))(routes_keys, routes_turns).reshape((TOKENS_B, TOPK))
    route_weight = jnp.clip(jnp.exp(math.log(1.0) - 2.3025851 * jax.random.uniform(key_list[13], (TOKENS_B, TOPK), jnp.float32) ** levels(key_list[13], (TOKENS_B, TOPK), ((0, 128),), -0.2, 0.2)), 0.1, 1.0)
    gate_w = noise(key_list[14], (EXPERTS, D, FF), D ** -0.5, 0.125, ((0, 16), (2, 8)))
    up_w = noise(key_list[15], (EXPERTS, D, FF), D ** -0.5, 0.125, ((0, 16), (2, 8)))
    down_w = noise(key_list[16], (EXPERTS, FF, D), FF ** -0.5, 0.125, ((0, 16), (1, 8)))
    return dict(query_latent=query_latent, kv_latent=kv_latent, rope_key=rope_key, query_gain=query_gain, kv_gain=kv_gain, query_nope_w=query_nope_w, query_rope_w=query_rope_w, key_up_w=key_up_w, value_up_w=value_up_w, output_w=output_w, expert_in=expert_in, moe_gain=moe_gain, routes=routes, route_weight=route_weight, gate_w=gate_w, up_w=up_w, down_w=down_w)


THETA = 10000.0

def rms_scale(values, gain):
    floats = values.astype(jnp.float32)
    square = lax.optimization_barrier(jnp.mean(floats * floats, axis=-1, keepdims=True))
    return (floats * lax.rsqrt(square + 1e-06) * gain).astype(jnp.bfloat16)

def rotate(values, positions):
    width = values.shape[-1]
    half = width // 2
    freq = 1.0 / THETA ** (jnp.arange(half, dtype=jnp.float32) * 2.0 / width)
    angle = positions.astype(jnp.float32)[:, None] * freq[None, :]
    angle = jnp.concatenate([angle, angle], axis=-1)
    cosine = jnp.cos(angle)
    sine = jnp.sin(angle)
    if values.ndim == 3:
        cosine = cosine[:, None, :]
        sine = sine[:, None, :]
    first = values[..., :half]
    second = values[..., half:]
    turned = jnp.concatenate([-second, first], axis=-1)
    return values * cosine + turned * sine

def expert_rows(rows, gate_one, up_one, down_one):
    gate = jnp.minimum(jnp.dot(rows, gate_one, preferred_element_type=jnp.float32), 7.0)
    upper = jnp.clip(jnp.dot(rows, up_one, preferred_element_type=jnp.float32), -7.0, 7.0)
    hidden = (gate * jax.nn.sigmoid(1.702 * gate) * (upper + 1.0)).astype(jnp.bfloat16)
    count = rows.shape[0]
    slices = hidden.reshape(count, N_TP, FF // N_TP).astype(jnp.float32)
    downs = down_one.reshape(N_TP, FF // N_TP, D).astype(jnp.float32)
    parts = jnp.einsum('rsf,sfd->srd', slices, downs)
    parts = lax.optimization_barrier(parts.astype(jnp.bfloat16)).astype(jnp.float32)
    return lax.optimization_barrier(jnp.sum(parts, axis=0)).astype(jnp.bfloat16)

def reference(query_latent, kv_latent, rope_key, query_gain, kv_gain, query_nope_w, query_rope_w, key_up_w, value_up_w, output_w, expert_in, moe_gain, routes, route_weight, gate_w, up_w, down_w):
    length = query_latent.shape[0]
    positions = jnp.arange(length, dtype=jnp.int32)
    query_normed = rms_scale(query_latent, query_gain)
    kv_normed = rms_scale(kv_latent, kv_gain)
    query_flat = jnp.dot(query_normed, query_nope_w, preferred_element_type=jnp.float32).astype(jnp.bfloat16)
    key_flat = jnp.dot(kv_normed, key_up_w, preferred_element_type=jnp.float32).astype(jnp.bfloat16)
    value_flat = jnp.dot(kv_normed, value_up_w, preferred_element_type=jnp.float32).astype(jnp.bfloat16)
    query_turn = jnp.dot(query_normed, query_rope_w, preferred_element_type=jnp.float32).reshape(length, HEADS, ROPE)
    query_rot = rotate(query_turn, positions).astype(jnp.bfloat16)
    key_rot = rotate(rope_key.astype(jnp.float32), positions).astype(jnp.bfloat16)
    queries = jnp.concatenate([query_flat.reshape(length, HEADS, NOPE), query_rot], axis=-1).astype(jnp.float32)
    keys = jnp.concatenate([key_flat.reshape(length, HEADS, NOPE), jnp.broadcast_to(key_rot[:, None, :], (length, HEADS, ROPE))], axis=-1).astype(jnp.float32)
    values = value_flat.reshape(length, HEADS, VDIM).astype(jnp.float32)
    block = math.gcd(length, 512)
    scale = 1.0 / math.sqrt(NOPE + ROPE)

    def attend(start):
        query_block = lax.dynamic_slice_in_dim(queries, start, block, 0)
        scores = jnp.einsum('qhd,khd->hqk', query_block, keys) * scale
        allowed = positions[None, :] <= (start + jnp.arange(block, dtype=jnp.int32))[:, None]
        masked = jnp.where(allowed[None], scores, -1e+30)
        peak = lax.optimization_barrier(jnp.max(masked, axis=-1, keepdims=True))
        expo = jnp.where(allowed[None], jnp.exp(masked - peak), 0.0)
        total = lax.optimization_barrier(jnp.sum(expo, axis=-1))
        probs = expo.astype(jnp.bfloat16).astype(jnp.float32)
        summed = jnp.einsum('hqk,khd->qhd', probs, values)
        return (summed / jnp.transpose(total)[:, :, None]).astype(jnp.bfloat16)
    starts = jnp.arange(length // block, dtype=jnp.int32) * block
    attended = lax.map(attend, starts).reshape(length, HEADS * VDIM)
    group = HEADS * VDIM // N_TP
    mixed = jnp.zeros((length, D), jnp.float32)
    for index in range(N_TP):
        part = jnp.dot(attended[:, index * group:(index + 1) * group], output_w[index * group:(index + 1) * group], preferred_element_type=jnp.float32)
        mixed = mixed + lax.optimization_barrier(part.astype(jnp.bfloat16)).astype(jnp.float32)
    mixer_out = mixed.astype(jnp.bfloat16)
    floats = expert_in.astype(jnp.float32)
    center = floats - lax.optimization_barrier(jnp.mean(floats, axis=-1, keepdims=True))
    variance = lax.optimization_barrier(jnp.mean(center * center, axis=-1, keepdims=True))
    normed_in = (center * lax.rsqrt(variance + 1e-05) * moe_gain).astype(jnp.bfloat16)
    tokens_b = expert_in.shape[0]
    flat = routes.reshape(-1).astype(jnp.int32)
    assigned = flat.shape[0]
    owner = (jnp.arange(assigned, dtype=jnp.int32) // TOPK).astype(jnp.int32)
    weights = route_weight / lax.optimization_barrier(jnp.sum(route_weight, axis=-1, keepdims=True))
    flat_weight = weights.reshape(-1)
    order = jnp.argsort(flat, stable=True).astype(jnp.int32)
    counts = lax.optimization_barrier(jnp.sum((flat[:, None] == jnp.arange(EXPERTS, dtype=jnp.int32)[None, :]).astype(jnp.int32), axis=0))
    firsts = (jnp.cumsum(counts) - counts).astype(jnp.int32)
    most_rows = N_EP * N_TP * CAP

    def per_expert(total, expert):
        offsets = jnp.arange(most_rows, dtype=jnp.int32)
        valid = offsets < counts[expert]
        index = jnp.minimum(firsts[expert] + offsets, assigned - 1).astype(jnp.int32)
        picked = order[index]
        rows = normed_in[owner[picked]]
        result = expert_rows(rows, gate_w[expert], up_w[expert], down_w[expert])
        factor = jnp.where(valid, flat_weight[picked], 0.0)
        total = total.at[owner[picked]].add(factor[:, None] * result.astype(jnp.float32))
        return (total, None)
    combined, unused = lax.scan(per_expert, jnp.zeros((tokens_b, D), jnp.float32), jnp.arange(EXPERTS, dtype=jnp.int32))
    return (mixer_out, combined.astype(jnp.bfloat16))
```

```python
import functools
import math

import jax
import jax.numpy as jnp
from jax import lax
from jax.experimental import pallas as pl
from jax.experimental.pallas import tpu as pltpu
from jax.sharding import PartitionSpec as P

BF = jnp.bfloat16
F32 = jnp.float32
NOPE, ROPE, VDIM = 128, 64, 128
QLAT, KVLAT, D = 768, 512, 2048
HID = 256
TOK = 128
GROUP = 1024
HALF = 512
LAT = QLAT + KVLAT + 128
KVR = HALF + HALF + HALF // 2
KVH = KVR // 2
QT = 256
THETA = 10000.0
MESH = pl.DeviceIdType.MESH
SCALE2 = math.log2(math.e) / math.sqrt(NOPE + ROPE)
VM = pltpu.VMEM


def dot(a, b):
    return jnp.dot(a, b, preferred_element_type=F32)


def kernel(
    ql_ref, kl_ref, kr_ref, qg_ref, kg_ref, ct_ref, st_ref, wq_ref, wr_ref, wk_ref, wv_ref,
    xin_ref, mg_ref, routes_ref, rw_ref, ow_hbm, gw_hbm, uw_hbm, dw_hbm,
    omix_ref, oexp_ref,
    lat, kv, qa, qb, m_s, l_s, acc, att_loc, att_snd, att_rcv,
    ow, gw, uw, dw,
    out, xb, bb, back, pp, ra, rb, rc, sb,
    pm, ma, mb, mc, ms, sid_s, nrm,
    loc_sem, m1_s, m1_r, w_s, w_r, a1_s, a1_r, d1_s, d1_r,
    p1_s, p1_r, p2_s, p2_r, x1_s, x1_r, x2_s, x2_r,
    r_s, r_r, t_s, t_r, at_s, at_r, m5_s, m5_r,
):
    ep = lax.axis_index("ep")
    tp = lax.axis_index("tp")
    y, core = tp // 2, tp % 2
    z, x = ep // 4, ep % 4
    mate = {"ep": ep, "tp": y * 2 + 1 - core}

    def wrap(a):
        return (a + 4) % 4

    def at_y(dy):
        return {"ep": ep, "tp": wrap(y + dy) * 2 + core}

    def at_ep(e):
        return {"ep": e, "tp": tp}

    def remote(src, dst, ssem, rsem, dev):
        return pltpu.make_async_remote_copy(
            src_ref=src, dst_ref=dst, send_sem=ssem, recv_sem=rsem, device_id=dev, device_id_type=MESH
        )

    barrier = pltpu.get_barrier_semaphore()
    for dy in (1, 2, 3):
        pl.semaphore_signal(barrier, inc=1, device_id=at_y(dy), device_id_type=MESH)
    pl.semaphore_signal(barrier, inc=1, device_id=mate, device_id_type=MESH)

    def greet(k, c):
        pl.semaphore_signal(barrier, inc=1, device_id=at_ep((ep + k) % 16), device_id_type=MESH)
        return c

    lax.fori_loop(1, 16, greet, 0)

    locals_ = [
        pltpu.make_async_copy(gw_hbm, gw.at[0], loc_sem.at[0]),
        pltpu.make_async_copy(uw_hbm, uw.at[0], loc_sem.at[1]),
        pltpu.make_async_copy(dw_hbm, dw.at[0], loc_sem.at[2]),
        pltpu.make_async_copy(ow_hbm, ow.at[0], loc_sem.at[3]),
    ]
    for c in locals_:
        c.start()

    f = xin_ref[...].astype(F32)
    cen = f - jnp.mean(f, axis=-1, keepdims=True)
    var = jnp.mean(cen * cen, axis=-1, keepdims=True)
    nrm[...] = (cen * lax.rsqrt(var + 1e-05) * mg_ref[...]).astype(BF)
    routes = routes_ref[...]
    r0, r1 = routes[:, 0:1], routes[:, 1:2]
    lane = lax.broadcasted_iota(jnp.int32, (TOK, 128), 1)
    oh0 = jnp.where(lane == r0, 1.0, 0.0).astype(F32)
    oh1 = jnp.where(lane == r1, 1.0, 0.0).astype(F32)
    before = lax.broadcasted_iota(jnp.int32, (TOK, TOK), 0) > lax.broadcasted_iota(jnp.int32, (TOK, TOK), 1)
    prior = dot(jnp.where(before, 1.0, 0.0).astype(BF), (oh0 + oh1).astype(BF))

    def slot_of(r, oh):
        rank = jnp.sum(prior * oh, axis=1, keepdims=True)
        one = (r & 1).astype(F32)
        grp = (r >> 1).astype(F32)
        low = one * 128.0 + grp * 8.0 + rank
        high = 256.0 + grp * 8.0 + one * 2.0 + rank - 8.0
        return jnp.where(rank < 8.0, low, high)

    s0, s1 = slot_of(r0, oh0), slot_of(r1, oh1)
    sid_s[0] = jnp.broadcast_to(s0, (TOK, 128))
    sid_s[1] = jnp.broadcast_to(s1, (TOK, 128))
    slots = lax.broadcasted_iota(jnp.int32, (TOK, 384), 1).astype(F32)
    sel = jnp.where((slots == s0) | (slots == s1), 1.0, 0.0).astype(BF)
    for n in range(4):
        cols = slice(n * 512, n * 512 + 512)
        got = lax.dot_general(sel, nrm[:, cols], (((0,), (0,)), ((), ())), preferred_element_type=F32)
        out[:, :, cols] = got.reshape(48, 8, 512).astype(BF)

    def rms(ref, gain):
        v = ref[...].astype(F32)
        sq = jnp.mean(v * v, axis=-1, keepdims=True)
        return (v * lax.rsqrt(sq + 1e-06) * gain[...]).astype(BF)

    lat[tp, :, 0:QLAT] = rms(ql_ref, qg_ref)
    lat[tp, :, QLAT:QLAT + KVLAT] = rms(kl_ref, kg_ref)
    lat[tp, :, QLAT + KVLAT:LAT] = kr_ref[...]

    pl.semaphore_wait(barrier, 19)

    def m1(k, c):
        dst = (ep + k) % 16
        for e in range(2):
            remote(out.at[e * 16 + dst], xb.at[y, e, ep], m1_s.at[e], m1_r.at[e], at_ep(dst)).start()
        remote(out.at[32 + dst], bb.at[ep], m1_s.at[2], m1_r.at[2], at_ep(dst)).start()
        return c

    lax.fori_loop(1, 16, m1, 0)
    for e in range(2):
        xb[y, e, ep] = out[e * 16 + ep]
    bb[ep] = out[32 + ep]

    a1 = [remote(lat.at[tp], lat.at[tp], a1_s.at[dy - 1], a1_r.at[dy - 1], at_y(dy)) for dy in (1, 2, 3)]
    for c in (a1[0], a1[2], a1[1]):
        c.start()
    d1 = [remote(lat.at[tp], lat.at[tp], d1_s.at[0], d1_r.at[0], mate)]
    d1[0].start()
    ws = [
        remote(gw_hbm, gw.at[1], w_s.at[0], w_r.at[0], mate),
        remote(uw_hbm, uw.at[1], w_s.at[1], w_r.at[1], mate),
        remote(dw_hbm, dw.at[1], w_s.at[2], w_r.at[2], mate),
        remote(ow_hbm, ow.at[1], w_s.at[3], w_r.at[3], mate),
    ]
    for c in ws:
        c.start()
    for dy in (1, 3, 2):
        a1[dy - 1].wait_recv()
        t = wrap(y - dy) * 2 + core
        c = remote(lat.at[t], lat.at[t], d1_s.at[dy], d1_r.at[dy], mate)
        c.start()
        d1.append(c)
    for c in d1:
        c.wait_recv()

    lane128 = lax.broadcasted_iota(jnp.int32, (HALF // 2, 128), 1)
    lane512 = lax.broadcasted_iota(jnp.int32, (HALF, 128), 1)
    for h in range(2):
        part = lat[h * 4:h * 4 + 4]
        qn = part[:, :, 0:QLAT].reshape(HALF, QLAT)
        kvn = part[:, :, QLAT:QLAT + KVLAT].reshape(HALF, KVLAT)
        rows = slice(h * HALF, h * HALF + HALF)
        qf = dot(qn, wq_ref[...])
        tt = dot(qn, wr_ref[...])
        rot = (tt * ct_ref[rows] + pltpu.roll(tt, 64, 1) * st_ref[rows]).astype(BF)
        zero = jnp.zeros_like(rot)
        qa[rows, 0:128] = qf.astype(BF)
        qb[rows, 0:128] = qf.astype(BF)
        qa[rows, 128:256] = jnp.where(lane512 < 64, rot, zero)
        qb[rows, 128:256] = jnp.where(lane512 < 64, zero, rot)
        kv[h, ep, 0:HALF] = dot(kvn, wk_ref[...]).astype(BF)
        kv[h, ep, HALF:2 * HALF] = dot(kvn, wv_ref[...]).astype(BF)
        lo = part[0:2, :, QLAT + KVLAT:LAT].reshape(HALF // 2, 128)
        hi = part[2:4, :, QLAT + KVLAT:LAT].reshape(HALF // 2, 128)
        kv[h, ep, 2 * HALF:KVR] = jnp.where(lane128 < 64, lo, hi)

    def slot(h, du, dv):
        if h == 0:
            return wrap(z + dv) * 4 + wrap(x + du)
        return wrap(z + du) * 4 + wrap(x + dv)

    pieces = (slice(0, KVH), slice(KVH, KVR))
    signs = (1, -1)
    order = (0, -1, 1, 2)
    P1, P1F, P2, P2F = {}, {}, {}, {}
    for h in range(2):
        for d in range(2):
            sg = signs[d]
            own = kv.at[h, slot(h, 0, 0)]
            P1[h, d] = remote(own, own, p1_s.at[h, d], p1_r.at[h, d], at_ep(slot(h, sg, 0)))
            fw = kv.at[h, slot(h, -sg, 0), pieces[d]]
            P1F[h, d] = remote(fw, fw, p1_s.at[h, 2 + d], p1_r.at[h, 2 + d], at_ep(slot(h, sg, 0)))
            for i in range(4):
                own = kv.at[h, slot(h, order[i], 0)]
                P2[h, i, d] = remote(own, own, p2_s.at[h, i, d], p2_r.at[h, i, d], at_ep(slot(h, 0, sg)))
                fw = kv.at[h, slot(h, order[i], -sg), pieces[d]]
                P2F[h, i, d] = remote(fw, fw, p2_s.at[h, i, 2 + d], p2_r.at[h, i, 2 + d], at_ep(slot(h, 0, sg)))

    for h in range(2):
        for d in range(2):
            P1[h, d].start()
        for d in range(2):
            P2[h, 0, d].start()

    for e in range(2):
        rep = xb.at[y, e, pl.ds(0, 15)]
        remote(rep, rep, m1_s.at[e], m1_r.at[e], mate).wait()
    rep = bb.at[pl.ds(0, 15)]
    remote(rep, rep, m1_s.at[2], m1_r.at[2], mate).wait()
    row64 = lax.broadcasted_iota(jnp.int32, (64, 128), 0)
    col128 = lax.broadcasted_iota(jnp.int32, (64, 128), 1)
    want = ((row64 & 31) >> 1) * 8 + (row64 >> 5) * 2 + (row64 & 1)
    squeeze = jnp.where(want == col128, 1.0, 0.0).astype(BF)
    for n in range(4):
        cols = slice(n * 512, n * 512 + 512)
        both = bb[:, :, cols].reshape(128, 512)
        tight = dot(squeeze, both).reshape(8, 8, 512).astype(BF)
        for e in range(2):
            xb[y, e, 16:20, :, cols] = tight[e * 4:e * 4 + 4]
    X1, X2 = [], []
    for d in range(2):
        X1.append(remote(xb.at[y], xb.at[y], x1_s.at[d], x1_r.at[d], at_y(signs[d])))
        fw = xb.at[wrap(y - signs[d]), d]
        X2.append(remote(fw, fw, x2_s.at[d], x2_r.at[d], at_y(signs[d])))
    for c in X1:
        c.start()

    def step(h, src, qi, masked):
        rows = pl.ds(pl.multiple_of(qi * QT, QT), QT)
        keys0 = kv[h, src, 0:256]
        keys1 = kv[h, src, 256:512]
        rots = kv[h, src, 2 * HALF:KVR]
        vals = kv[h, src, HALF:2 * HALF]
        nt = (((1,), (1,)), ((), ()))
        sa = lax.dot_general(qa[rows], jnp.concatenate([keys0, rots], 1), nt, preferred_element_type=F32)
        sb_ = lax.dot_general(qb[rows], jnp.concatenate([keys1, rots], 1), nt, preferred_element_type=F32)
        s = jnp.concatenate([sa, sb_], 1) * SCALE2
        if masked:
            qp = qi * QT + lax.broadcasted_iota(jnp.int32, (QT, HALF), 0)
            kp = h * HALF + lax.broadcasted_iota(jnp.int32, (QT, HALF), 1)
            s = jnp.where(kp <= qp, s, -1e30)
        old = m_s[rows]
        new = jnp.maximum(old, jnp.max(s, axis=1, keepdims=True))
        p = jnp.exp2(s - new[:, 0:1])
        fac = jnp.exp2(old - new)
        m_s[rows] = new
        l_s[rows] = l_s[rows] * fac + ((p[:, 0:128] + p[:, 128:256]) + (p[:, 256:384] + p[:, 384:512]))
        acc[rows] = acc[rows] * fac + dot(p.astype(BF), vals)

    def attend(h, src):
        @pl.when(src < ep)
        def _():
            lax.fori_loop(0, GROUP // QT, lambda qi, c: (step(h, src, qi, False), c)[1], 0)

    m_s[...] = jnp.full((GROUP, 128), -1e30, F32)
    l_s[...] = jnp.zeros((GROUP, 128), F32)
    acc[...] = jnp.zeros((GROUP, 128), F32)
    lax.fori_loop(0, 4, lambda qi, c: (step(0, ep, qi, True), c)[1], 0)
    lax.fori_loop(2, 4, lambda qi, c: (step(1, ep, qi, True), c)[1], 0)

    for h in range(2):
        for d in range(2):
            P1[h, d].wait_recv()
            P1F[h, d].start()
        for i in (1, 2):
            for d in range(2):
                P2[h, i, d].start()

    for c in locals_:
        c.wait()
    for c in ws:
        c.wait_recv()

    def expert(ys):
        n = len(ys)

        def one(e, c):
            rows = jnp.concatenate([xb[b, e].reshape(160, D) for b in ys], 0)
            total = [None] * 4
            hid = []
            for w in range(2):
                g = jnp.minimum(dot(rows, gw[w, e]), 7.0)
                u = jnp.clip(dot(rows, uw[w, e]), -7.0, 7.0)
                hid.append((g * jax.nn.sigmoid(1.702 * g) * (u + 1.0)).astype(BF))
            both = jnp.concatenate(hid, 1)
            for q in range(4):
                cols = slice(q * 512, q * 512 + 512)
                down = jnp.concatenate([dw[0, e, :, cols], dw[1, e, :, cols]], 0)
                total = dot(both, down).astype(BF)
                for k in range(n):
                    pp[ys[k], e, :, cols] = total[k * 160:k * 160 + 160]
            return c

        lax.fori_loop(0, 2, one, 0)

    def ring(part, a_, b_, c_, s_, ssem, rsem):
        C, A, B = [], [], []
        for d in range(2):
            dev = at_y(signs[d])
            near = wrap(y + signs[d])
            far = wrap(y + 2)
            C.append(remote(part.at[near, 1 - d], c_.at[d], ssem.at[d], rsem.at[d], dev))
            A.append(remote(part.at[far, d], a_.at[d], ssem.at[2 + d], rsem.at[2 + d], dev))
            B.append(remote(s_.at[d], b_.at[d], ssem.at[4 + d], rsem.at[4 + d], dev))
        return C, A, B

    def relay(part, a_, s_, A, B):
        for d in range(2):
            A[d].wait_recv()
            s_[d] = (part[wrap(y + signs[d]), d].astype(F32) + a_[d].astype(F32)).astype(BF)
            B[d].start()

    RC, RA, RB = ring(pp, ra, rb, rc, sb, r_s, r_r)
    TC, TA, TB = ring(pm, ma, mb, mc, ms, t_s, t_r)

    expert([y])

    for h in range(2):
        for d in range(2):
            P1F[h, d].wait_recv()
        for d in range(2):
            P2[h, 3, d].start()
    for h in range(2):
        for du in (-1, 1):
            attend(h, slot(h, du, 0))
    for d in range(2):
        X1[d].wait_recv()
        X2[d].start()
    for h in range(2):
        for d in range(2):
            P2[h, 0, d].wait_recv()
            P2F[h, 0, d].start()
    expert([wrap(y + 1), wrap(y - 1)])
    for c in RC:
        c.start()
    for i in (1, 2):
        for h in range(2):
            for d in range(2):
                P2[h, i, d].wait_recv()
                P2F[h, i, d].start()
    for h in range(2):
        attend(h, slot(h, 2, 0))
        for dv in (-1, 1):
            attend(h, slot(h, 0, dv))
    for c in X2:
        c.wait_recv()
    expert([wrap(y + 2)])
    for c in RA:
        c.start()
    for h in range(2):
        for d in range(2):
            P2[h, 3, d].wait_recv()
            P2F[h, 3, d].start()
    for h in range(2):
        for i in (1, 2):
            for dv in (-1, 1):
                attend(h, slot(h, order[i], dv))
    relay(pp, ra, sb, RA, RB)
    for h in range(2):
        for dv in (-1, 1):
            attend(h, slot(h, 2, dv))
    for i in range(4):
        for h in range(2):
            for d in range(2):
                P2F[h, i, d].wait_recv()
            attend(h, slot(h, order[i], 2))

    for b in range(4):
        for side, dst in ((core, att_loc), (1 - core, att_snd)):
            rows = pl.ds(pl.multiple_of((b * 2 + side) * TOK, TOK), TOK)
            total = jnp.sum(l_s[rows], axis=1, keepdims=True)
            dst[b] = (acc[rows] / total).astype(BF)
    AT = remote(att_snd, att_rcv, at_s, at_r, mate)
    AT.start()
    AT.wait_recv()
    heads = jnp.concatenate([att_loc[...].reshape(HALF, VDIM), att_rcv[...].reshape(HALF, VDIM)], 1)
    for q in range(4):
        cols = slice(q * 512, q * 512 + 512)
        w2 = jnp.concatenate([ow[0, :, cols], ow[1, :, cols]], 0)
        pm[:, :, :, cols] = dot(heads, w2).astype(BF).reshape(4, 2, 64, 512)
    for c in TC + TA:
        c.start()

    final = []
    for e in range(2):
        RC[1 - e].wait_recv()
        RB[e].wait_recv()
        whole = pp[y, e].astype(F32) + rb[e].astype(F32) + rc[1 - e].astype(F32)
        tight = whole.astype(BF)
        final.append(tight[128:160])
        out[e * 16:e * 16 + 16] = tight[0:128].reshape(16, 8, D)
    compact = jnp.concatenate(final, 0)
    for n in range(4):
        cols = slice(n * 512, n * 512 + 512)
        wide = lax.dot_general(
            squeeze, compact[:, cols], (((0,), (0,)), ((), ())), preferred_element_type=F32
        )
        out[32:48, :, cols] = wide.reshape(16, 8, 512).astype(BF)

    def m5(k, c):
        dst = (ep + k) % 16
        for g in range(3):
            remote(out.at[g * 16 + dst], back.at[g * 16 + ep], m5_s.at[g], m5_r.at[g], at_ep(dst)).start()
        return c

    lax.fori_loop(1, 16, m5, 0)
    for g in range(3):
        back[g * 16 + ep] = out[g * 16 + ep]

    relay(pm, ma, ms, TA, TB)

    for g in range(3):
        rep = back.at[pl.ds(g * 16, 15)]
        remote(rep, rep, m5_s.at[g], m5_r.at[g], mate).wait()
    rw = rw_ref[...]
    tot = jnp.sum(rw, axis=1, keepdims=True)
    w0, w1 = rw[:, 0:1] / tot, rw[:, 1:2] / tot
    pick0 = jnp.where(slots == sid_s[0][:, 0:1], 1.0, 0.0).astype(BF)
    pick1 = jnp.where(slots == sid_s[1][:, 0:1], 1.0, 0.0).astype(BF)
    for n in range(4):
        cols = slice(n * 512, n * 512 + 512)
        rows = back[:, :, cols].reshape(384, 512)
        oexp_ref[:, cols] = (w0 * dot(pick0, rows) + w1 * dot(pick1, rows)).astype(BF)

    for e in range(2):
        TC[1 - e].wait_recv()
        TB[e].wait_recv()
        whole = pm[y, e].astype(F32) + mb[e].astype(F32) + mc[1 - e].astype(F32)
        omix_ref[e * 64:e * 64 + 64] = whole.astype(BF)

    for c in a1 + d1 + ws + X1 + X2 + RC + RA + RB + TC + TA + TB + [AT]:
        c.wait_send()
    for group in (P1, P1F, P2, P2F):
        for c in group.values():
            c.wait_send()


def tables(ep):
    half = ROPE // 2
    freq = 1.0 / THETA ** (jnp.arange(half, dtype=F32) * 2.0 / ROPE)
    positions = ep * GROUP + jnp.arange(GROUP, dtype=jnp.int32)
    angle = positions.astype(F32)[:, None] * freq[None, :]
    return jnp.cos(angle), jnp.sin(angle)


def per_device(
    query_latent, kv_latent, rope_key, query_gain, kv_gain, query_nope_w, query_rope_w,
    key_up_w, value_up_w, output_w, expert_in, moe_gain, routes, route_weight, gate_w, up_w, down_w,
):
    ep = lax.axis_index("ep")
    tp = lax.axis_index("tp")
    cosine, sine = tables(ep)
    cc = jnp.concatenate([cosine, cosine, sine, sine], 1)
    ss = jnp.concatenate([sine, sine, cosine, cosine], 1)
    mine = lax.dynamic_slice_in_dim(cc, tp * TOK, TOK, 0)
    cm, sm = mine[:, 0:64], mine[:, 64:128]
    rk = rope_key.astype(F32)
    turned = jnp.concatenate([-rk[:, 32:], rk[:, :32]], 1)
    kr = (rk * cm + turned * sm).astype(BF)
    kr = jnp.concatenate([kr, kr], 1)
    wr = jnp.concatenate([query_rope_w, -query_rope_w[:, 32:], query_rope_w[:, :32]], 1)
    dma = pltpu.SemaphoreType.DMA
    vm = pl.BlockSpec(memory_space=VM)
    hbm = pl.BlockSpec(memory_space=pl.ANY)
    return pl.pallas_call(
        kernel,
        out_shape=(jax.ShapeDtypeStruct((TOK, D), BF), jax.ShapeDtypeStruct((TOK, D), BF)),
        in_specs=[vm] * 15 + [hbm] * 4,
        out_specs=(vm, vm),
        scratch_shapes=[
            VM((8, TOK, LAT), BF), VM((2, 16, KVR, 128), BF), VM((GROUP, 256), BF), VM((GROUP, 256), BF),
            VM((GROUP, 128), F32), VM((GROUP, 128), F32), VM((GROUP, 128), F32),
            VM((4, TOK, 128), BF), VM((4, TOK, 128), BF), VM((4, TOK, 128), BF),
            VM((2, 128, D), BF), VM((2, 2, D, HID), BF), VM((2, 2, D, HID), BF), VM((2, 2, HID, D), BF),
            VM((48, 8, D), BF), VM((4, 2, 20, 8, D), BF), VM((16, 8, D), BF), VM((48, 8, D), BF),
            VM((4, 2, 160, D), BF), VM((2, 160, D), BF), VM((2, 160, D), BF), VM((2, 160, D), BF), VM((2, 160, D), BF),
            VM((4, 2, 64, D), BF), VM((2, 64, D), BF), VM((2, 64, D), BF), VM((2, 64, D), BF), VM((2, 64, D), BF),
            VM((2, TOK, 128), F32), VM((TOK, D), BF),
            dma((4,)), dma((3,)), dma((3,)), dma((4,)), dma((4,)), dma((3,)), dma((3,)), dma((4,)), dma((4,)),
            dma((2, 4)), dma((2, 4)), dma((2, 4, 4)), dma((2, 4, 4)), dma((2,)), dma((2,)), dma((2,)), dma((2,)),
            dma((6,)), dma((6,)), dma((6,)), dma((6,)), dma, dma, dma((3,)), dma((3,)),
        ],
        compiler_params=pltpu.CompilerParams(
            collective_id=0, has_side_effects=True, vmem_limit_bytes=66_000_000
        ),
    )(
        query_latent, kv_latent, kr, query_gain.reshape(1, -1), kv_gain.reshape(1, -1), cc, ss,
        query_nope_w, wr, key_up_w, value_up_w, expert_in, moe_gain.reshape(1, -1), routes, route_weight,
        output_w, gate_w, up_w, down_w,
    )


def solution(mesh):
    rows = P(("ep", "tp"), None)
    placed = (
        rows, rows, rows, P(), P(), P(None, "tp"), P(None, "tp"), P(None, "tp"), P(None, "tp"), P("tp", None),
        rows, P(), rows, rows, P("ep", None, "tp"), P("ep", None, "tp"), P("ep", "tp", None),
    )
    return jax.shard_map(per_device, mesh=mesh, in_specs=placed, out_specs=(rows, rows), check_vma=False)
```

```python
import functools
import math

import jax
import jax.numpy as jnp
import numpy as np
from jax import lax
from jax.experimental import pallas as pl
from jax.experimental.pallas import tpu as pltpu
from jax.sharding import PartitionSpec as P

BF = jnp.bfloat16
F32 = jnp.float32
NOPE, ROPE, VDIM = 128, 64, 128
QLAT, KVLAT, D = 768, 512, 2048
HID = 256
TOK = 128
GROUP = 1024
HALF = 512
LAT = QLAT + KVLAT + 128
KVR = HALF + HALF + HALF // 2
KVH = KVR // 2
QT = 256
THETA = 10000.0
MESH = pl.DeviceIdType.MESH
SCALE2 = math.log2(math.e) / math.sqrt(NOPE + ROPE)
VM = pltpu.VMEM


def dot(a, b):
    return jnp.dot(a, b, preferred_element_type=F32)


def kernel(
    ql_ref, kl_ref, rk_ref, qg_ref, kg_ref, tab_ref, wq_ref, wp_ref, wk_ref, wv_ref,
    xin_ref, mg_ref, routes_ref, rw_ref, ow_hbm, gw_hbm, uw_hbm, dw_hbm,
    omix_ref, oexp_ref,
    lat, kv, qa, qb, m_s, l_s, acc, att_loc, att_snd, att_rcv,
    ow, gw, uw, dw,
    out, outb, xb, bb, back, backb, pp, ra, rb, rc, sb,
    pm, ma, mb, mc, ms, sid_s, nrm,
    loc_sem, m1_s, m1_r, w_s, w_r, a1_s, a1_r, d1_s, d1_r,
    p1_s, p1_r, p2_s, p2_r, x1_s, x1_r, x2_s, x2_r,
    r_s, r_r, t_s, t_r, at_s, at_r, m5_s, m5_r,
):
    ep = lax.axis_index("ep")
    tp = lax.axis_index("tp")
    y, core = tp // 2, tp % 2
    z, x = ep // 4, ep % 4
    mate = {"ep": ep, "tp": y * 2 + 1 - core}

    def wrap(a):
        return (a + 4) % 4

    def at_y(dy):
        return {"ep": ep, "tp": wrap(y + dy) * 2 + core}

    def at_ep(e):
        return {"ep": e, "tp": tp}

    def remote(src, dst, ssem, rsem, dev):
        return pltpu.make_async_remote_copy(
            src_ref=src, dst_ref=dst, send_sem=ssem, recv_sem=rsem, device_id=dev, device_id_type=MESH
        )

    barrier = pltpu.get_barrier_semaphore()
    for dy in (1, 2, 3):
        pl.semaphore_signal(barrier, inc=1, device_id=at_y(dy), device_id_type=MESH)
    pl.semaphore_signal(barrier, inc=1, device_id=mate, device_id_type=MESH)

    def greet(k, c):
        pl.semaphore_signal(barrier, inc=1, device_id=at_ep((ep + k) % 16), device_id_type=MESH)
        return c

    lax.fori_loop(1, 16, greet, 0)

    locals_ = [
        pltpu.make_async_copy(gw_hbm, gw.at[0], loc_sem.at[0]),
        pltpu.make_async_copy(uw_hbm, uw.at[0], loc_sem.at[1]),
        pltpu.make_async_copy(dw_hbm, dw.at[0], loc_sem.at[2]),
        pltpu.make_async_copy(ow_hbm, ow.at[0], loc_sem.at[3]),
    ]
    for c in locals_:
        c.start()

    f = xin_ref[...].astype(F32)
    cen = f - jnp.mean(f, axis=-1, keepdims=True)
    var = jnp.mean(cen * cen, axis=-1, keepdims=True)
    nrm[...] = (cen * lax.rsqrt(var + 1e-05) * mg_ref[...]).astype(BF)
    rowi = lax.broadcasted_iota(jnp.int32, (TOK, TOK), 0)
    coli = lax.broadcasted_iota(jnp.int32, (TOK, TOK), 1)

    def column(row):
        return jnp.sum(jnp.where(rowi == coli, jnp.broadcast_to(row, (TOK, TOK)), 0.0), axis=1, keepdims=True)

    routes = routes_ref[...].astype(F32)
    r0, r1 = (column(routes[k:k + 1]).astype(jnp.int32) for k in range(2))
    lane = lax.broadcasted_iota(jnp.int32, (TOK, 128), 1)
    oh0 = jnp.where(lane == r0, 1.0, 0.0).astype(F32)
    oh1 = jnp.where(lane == r1, 1.0, 0.0).astype(F32)
    prior = dot(jnp.where(rowi > coli, 1.0, 0.0).astype(BF), (oh0 + oh1).astype(BF))

    def slot_of(r, oh):
        rank = jnp.sum(prior * oh, axis=1, keepdims=True)
        one = (r & 1).astype(F32)
        grp = (r >> 1).astype(F32)
        low = one * 128.0 + grp * 8.0 + rank
        high = 256.0 + grp * 4.0 + one * 2.0 + rank - 8.0
        return jnp.where(rank < 8.0, low, high)

    s0, s1 = slot_of(r0, oh0), slot_of(r1, oh1)
    sid_s[0] = jnp.broadcast_to(s0, (TOK, 128))
    sid_s[1] = jnp.broadcast_to(s1, (TOK, 128))
    slots = lax.broadcasted_iota(jnp.int32, (TOK, 256), 1).astype(F32)
    slotb = lax.broadcasted_iota(jnp.int32, (TOK, 64), 1).astype(F32) + 256.0
    sel = jnp.where((slots == s0) | (slots == s1), 1.0, 0.0).astype(BF)
    selb = jnp.where((slotb == s0) | (slotb == s1), 1.0, 0.0).astype(BF)
    tn = (((0,), (0,)), ((), ()))
    for n in range(4):
        cols = slice(n * 512, n * 512 + 512)
        got = lax.dot_general(sel, nrm[:, cols], tn, preferred_element_type=F32)
        out[:, :, cols] = got.reshape(32, 8, 512).astype(BF)
        got = lax.dot_general(selb, nrm[:, cols], tn, preferred_element_type=F32)
        outb[:, :, cols] = got.reshape(16, 4, 512).astype(BF)

    def rms(ref, gain):
        v = ref[...].astype(F32)
        sq = jnp.mean(v * v, axis=-1, keepdims=True)
        return (v * lax.rsqrt(sq + 1e-06) * gain).astype(BF)

    lat[tp, :, 0:QLAT] = rms(ql_ref, qg_ref[...].reshape(1, QLAT))
    lat[tp, :, QLAT:QLAT + KVLAT] = rms(kl_ref, kg_ref[...])
    i64 = lax.broadcasted_iota(jnp.int32, (ROPE, 128), 0)
    j64 = lax.broadcasted_iota(jnp.int32, (ROPE, 128), 1)
    plain = jnp.where(i64 == j64, 1.0, 0.0) + jnp.where(i64 + 96 == j64, 1.0, 0.0)
    turn = (plain - jnp.where(i64 + 32 == j64, jnp.where(j64 >= 64, 1.0, 0.0), 0.0)).astype(BF)

    def angles(block):
        cb, sb0 = tab_ref[0], tab_ref[1]
        k = [tab_ref[2 + n, pl.ds(block, 1), :] for n in range(4)]
        return cb * k[0] + sb0 * k[1], cb * k[2] + sb0 * k[3]

    def rotated(both, ct, st):
        return (both * ct + pltpu.roll(both, 64, 1) * st).astype(BF)

    lat[tp, :, QLAT + KVLAT:LAT] = rotated(
        lax.dot_general(rk_ref[...], turn, tn, preferred_element_type=F32), *angles(ep * 8 + tp)
    )
    wr = lax.dot_general(wp_ref[...], turn, tn, preferred_element_type=F32).astype(BF)

    pl.semaphore_wait(barrier, 19)

    def m1(k, c):
        dst = (ep + k) % 16
        for e in range(2):
            remote(out.at[e * 16 + dst], xb.at[y, e, ep], m1_s.at[e], m1_r.at[e], at_ep(dst)).start()
        remote(outb.at[dst], bb.at[ep], m1_s.at[2], m1_r.at[2], at_ep(dst)).start()
        return c

    lax.fori_loop(1, 16, m1, 0)
    for e in range(2):
        xb[y, e, ep] = out[e * 16 + ep]
    bb[ep] = outb[ep]

    a1 = [remote(lat.at[tp], lat.at[tp], a1_s.at[dy - 1], a1_r.at[dy - 1], at_y(dy)) for dy in (1, 2, 3)]
    for c in (a1[0], a1[2], a1[1]):
        c.start()
    d1 = [remote(lat.at[tp], lat.at[tp], d1_s.at[0], d1_r.at[0], mate)]
    d1[0].start()
    ws = [
        remote(gw_hbm, gw.at[1], w_s.at[0], w_r.at[0], mate),
        remote(uw_hbm, uw.at[1], w_s.at[1], w_r.at[1], mate),
        remote(dw_hbm, dw.at[1], w_s.at[2], w_r.at[2], mate),
        remote(ow_hbm, ow.at[1], w_s.at[3], w_r.at[3], mate),
    ]
    for c in ws:
        c.start()
    for dy in (1, 3, 2):
        a1[dy - 1].wait_recv()
        t = wrap(y - dy) * 2 + core
        c = remote(lat.at[t], lat.at[t], d1_s.at[dy], d1_r.at[dy], mate)
        c.start()
        d1.append(c)
    for c in d1:
        c.wait_recv()

    lane128 = lax.broadcasted_iota(jnp.int32, (HALF // 2, 128), 1)
    lane512 = lax.broadcasted_iota(jnp.int32, (HALF, 128), 1)
    for h in range(2):
        part = lat[h * 4:h * 4 + 4]
        qn = part[:, :, 0:QLAT].reshape(HALF, QLAT)
        kvn = part[:, :, QLAT:QLAT + KVLAT].reshape(HALF, KVLAT)
        rows = slice(h * HALF, h * HALF + HALF)
        qf = dot(qn, wq_ref[...])
        tabs = [angles(ep * 8 + h * 4 + t) for t in range(4)]
        rot = rotated(
            dot(qn, wr), jnp.concatenate([t[0] for t in tabs], 0), jnp.concatenate([t[1] for t in tabs], 0)
        )
        zero = jnp.zeros_like(rot)
        qa[rows, 0:128] = qf.astype(BF)
        qb[rows, 0:128] = qf.astype(BF)
        qa[rows, 128:256] = jnp.where(lane512 < 64, rot, zero)
        qb[rows, 128:256] = jnp.where(lane512 < 64, zero, rot)
        kv[h, ep, 0:HALF] = dot(kvn, wk_ref[...]).astype(BF)
        kv[h, ep, HALF:2 * HALF] = dot(kvn, wv_ref[...]).astype(BF)
        lo = part[0:2, :, QLAT + KVLAT:LAT].reshape(HALF // 2, 128)
        hi = part[2:4, :, QLAT + KVLAT:LAT].reshape(HALF // 2, 128)
        kv[h, ep, 2 * HALF:KVR] = jnp.where(lane128 < 64, lo, hi)

    def slot(h, du, dv):
        if h == 0:
            return wrap(z + dv) * 4 + wrap(x + du)
        return wrap(z + du) * 4 + wrap(x + dv)

    pieces = (slice(0, KVH), slice(KVH, KVR))
    signs = (1, -1)
    order = (0, -1, 1, 2)
    P1, P1F, P2, P2F = {}, {}, {}, {}
    for h in range(2):
        for d in range(2):
            sg = signs[d]
            own = kv.at[h, slot(h, 0, 0)]
            P1[h, d] = remote(own, own, p1_s.at[h, d], p1_r.at[h, d], at_ep(slot(h, sg, 0)))
            fw = kv.at[h, slot(h, -sg, 0), pieces[d]]
            P1F[h, d] = remote(fw, fw, p1_s.at[h, 2 + d], p1_r.at[h, 2 + d], at_ep(slot(h, sg, 0)))
            for i in range(4):
                own = kv.at[h, slot(h, order[i], 0)]
                P2[h, i, d] = remote(own, own, p2_s.at[h, i, d], p2_r.at[h, i, d], at_ep(slot(h, 0, sg)))
                fw = kv.at[h, slot(h, order[i], -sg), pieces[d]]
                P2F[h, i, d] = remote(fw, fw, p2_s.at[h, i, 2 + d], p2_r.at[h, i, 2 + d], at_ep(slot(h, 0, sg)))

    for h in range(2):
        for d in range(2):
            P1[h, d].start()
        for d in range(2):
            P2[h, 0, d].start()

    for e in range(2):
        rep = xb.at[y, e, pl.ds(0, 15)]
        remote(rep, rep, m1_s.at[e], m1_r.at[e], mate).wait()
    rep = bb.at[pl.ds(0, 15)]
    remote(rep, rep, m1_s.at[2], m1_r.at[2], mate).wait()
    row64 = lax.broadcasted_iota(jnp.int32, (64, 64), 0)
    col64 = lax.broadcasted_iota(jnp.int32, (64, 64), 1)
    want = ((row64 & 31) >> 1) * 4 + (row64 >> 5) * 2 + (row64 & 1)
    squeeze = jnp.where(want == col64, 1.0, 0.0).astype(BF)
    for n in range(4):
        cols = slice(n * 512, n * 512 + 512)
        both = bb[:, :, cols].reshape(64, 512)
        tight = dot(squeeze, both).reshape(8, 8, 512).astype(BF)
        for e in range(2):
            xb[y, e, 16:20, :, cols] = tight[e * 4:e * 4 + 4]
    X1, XL, X2 = [], [], []
    for d in range(2):
        first, last = xb.at[y, d], xb.at[y, 1 - d]
        X1.append(remote(first, first, x1_s.at[d], x1_r.at[d], at_y(signs[d])))
        XL.append(remote(last, last, x1_s.at[2 + d], x1_r.at[2 + d], at_y(signs[d])))
        fw = xb.at[wrap(y - signs[d]), d]
        X2.append(remote(fw, fw, x2_s.at[d], x2_r.at[d], at_y(signs[d])))
    for c in X1:
        c.start()

    def step(h, src, qi, masked):
        rows = pl.ds(pl.multiple_of(qi * QT, QT), QT)
        keys0 = kv[h, src, 0:256]
        keys1 = kv[h, src, 256:512]
        rots = kv[h, src, 2 * HALF:KVR]
        vals = kv[h, src, HALF:2 * HALF]
        nt = (((1,), (1,)), ((), ()))
        sa = lax.dot_general(qa[rows], jnp.concatenate([keys0, rots], 1), nt, preferred_element_type=F32)
        sb_ = lax.dot_general(qb[rows], jnp.concatenate([keys1, rots], 1), nt, preferred_element_type=F32)
        s = jnp.concatenate([sa, sb_], 1) * SCALE2
        if masked:
            qp = qi * QT + lax.broadcasted_iota(jnp.int32, (QT, HALF), 0)
            kp = h * HALF + lax.broadcasted_iota(jnp.int32, (QT, HALF), 1)
            s = jnp.where(kp <= qp, s, -1e30)
        old = m_s[rows]
        new = jnp.maximum(old, jnp.max(s, axis=1, keepdims=True))
        p = jnp.exp2(s - new[:, 0:1])
        fac = jnp.exp2(old - new)
        m_s[rows] = new
        l_s[rows] = l_s[rows] * fac + ((p[:, 0:128] + p[:, 128:256]) + (p[:, 256:384] + p[:, 384:512]))
        acc[rows] = acc[rows] * fac + dot(p.astype(BF), vals)

    def attend(h, src):
        @pl.when(src < ep)
        def _():
            lax.fori_loop(0, GROUP // QT, lambda qi, c: (step(h, src, qi, False), c)[1], 0)

    m_s[...] = jnp.full((GROUP, 128), -1e30, F32)
    l_s[...] = jnp.zeros((GROUP, 128), F32)
    acc[...] = jnp.zeros((GROUP, 128), F32)
    lax.fori_loop(0, 4, lambda qi, c: (step(0, ep, qi, True), c)[1], 0)
    lax.fori_loop(2, 4, lambda qi, c: (step(1, ep, qi, True), c)[1], 0)

    for c in XL:
        c.start()

    def expert(ys):
        n = len(ys)

        def one(e, c):
            rows = jnp.concatenate([xb[b, e].reshape(160, D) for b in ys], 0)
            total = [None] * 4
            hid = []
            for w in range(2):
                g = jnp.minimum(dot(rows, gw[w, e]), 7.0)
                u = jnp.clip(dot(rows, uw[w, e]), -7.0, 7.0)
                hid.append((g * jax.nn.sigmoid(1.702 * g) * (u + 1.0)).astype(BF))
            both = jnp.concatenate(hid, 1)
            for q in range(4):
                cols = slice(q * 512, q * 512 + 512)
                down = jnp.concatenate([dw[0, e, :, cols], dw[1, e, :, cols]], 0)
                total = dot(both, down).astype(BF)
                for k in range(n):
                    pp[ys[k], e, :, cols] = total[k * 160:k * 160 + 160]
            return c

        lax.fori_loop(0, 2, one, 0)

    def ring(part, a_, b_, c_, s_, ssem, rsem):
        n = part.shape[2] // 2
        C, A, B = [], [], []
        for d in range(2):
            dev = at_y(signs[d])
            near = wrap(y + signs[d])
            far = wrap(y + 2)
            C.append(remote(part.at[near, 1 - d], c_.at[d], ssem.at[d], rsem.at[d], dev))
            for k in range(2):
                q = pl.ds(k * n, n)
                m = 2 + d * 2 + k
                A.append(remote(part.at[far, d, q], a_.at[d, q], ssem.at[m], rsem.at[m], dev))
                m = 6 + d * 2 + k
                B.append(remote(s_.at[d, q], b_.at[d, q], ssem.at[m], rsem.at[m], dev))
        return C, A, B

    def relay(part, a_, s_, A, B, k):
        n = part.shape[2] // 2
        q = slice(k * n, k * n + n)
        for d in range(2):
            A[d * 2 + k].wait_recv()
            s_[d, q] = (part[wrap(y + signs[d]), d, q].astype(F32) + a_[d, q].astype(F32)).astype(BF)
            B[d * 2 + k].start()

    RC, RA, RB = ring(pp, ra, rb, rc, sb, r_s, r_r)
    TC, TA, TB = ring(pm, ma, mb, mc, ms, t_s, t_r)

    def p1_on():
        for h in range(2):
            for d in range(2):
                P1[h, d].wait_recv()
                P1F[h, d].start()
        for h in range(2):
            for i in (1, 2):
                for d in range(2):
                    P2[h, i, d].start()

    def p2_on(i):
        for h in range(2):
            for d in range(2):
                P2[h, i, d].wait_recv()
                P2F[h, i, d].start()

    def p1f_on():
        for h in range(2):
            for d in range(2):
                P1F[h, d].wait_recv()
        for h in range(2):
            for d in range(2):
                P2[h, 3, d].start()

    def near(i):
        for h in range(2):
            for dv in (-1, 1):
                attend(h, slot(h, order[i], dv))

    def far(i):
        for h in range(2):
            for d in range(2):
                P2F[h, i, d].wait_recv()
            attend(h, slot(h, order[i], 2))

    for c in locals_:
        c.wait()
    for c in ws:
        c.wait_recv()
    expert([y])
    p1_on()
    p2_on(0)
    for c in X1:
        c.wait_recv()
    for c in X2:
        c.start()
    for h in range(2):
        for du in (-1, 1):
            attend(h, slot(h, du, 0))
    near(0)
    for c in XL:
        c.wait_recv()
    expert([wrap(y + 1), wrap(y - 1)])
    for c in RC:
        c.start()
    p1f_on()
    p2_on(1)
    p2_on(2)
    for h in range(2):
        attend(h, slot(h, 2, 0))
    near(1)
    for c in X2:
        c.wait_recv()
    expert([wrap(y + 2)])
    for k in (0, 2, 1, 3):
        RA[k].start()
    near(2)
    p2_on(3)
    near(3)
    far(0)
    relay(pp, ra, sb, RA, RB, 0)
    far(1)
    relay(pp, ra, sb, RA, RB, 1)
    far(2)
    far(3)

    for b in range(4):
        for side, dst in ((core, att_loc), (1 - core, att_snd)):
            rows = pl.ds(pl.multiple_of((b * 2 + side) * TOK, TOK), TOK)
            total = jnp.sum(l_s[rows], axis=1, keepdims=True)
            dst[b] = (acc[rows] / total).astype(BF)
    AT = remote(att_snd, att_rcv, at_s, at_r, mate)
    AT.start()
    AT.wait_recv()
    heads = jnp.concatenate([att_loc[...].reshape(HALF, VDIM), att_rcv[...].reshape(HALF, VDIM)], 1)
    for q in range(4):
        cols = slice(q * 512, q * 512 + 512)
        w2 = jnp.concatenate([ow[0, :, cols], ow[1, :, cols]], 0)
        pm[:, :, :, cols] = dot(heads, w2).astype(BF).reshape(4, 2, 64, 512)
    for c in TC:
        c.start()
    for k in (0, 2, 1, 3):
        TA[k].start()

    final = []
    for e in range(2):
        RC[1 - e].wait_recv()
        RB[e * 2].wait_recv()
        RB[e * 2 + 1].wait_recv()
        whole = pp[y, e].astype(F32) + rb[e].astype(F32) + rc[1 - e].astype(F32)
        tight = whole.astype(BF)
        final.append(tight[128:160])
        out[e * 16:e * 16 + 16] = tight[0:128].reshape(16, 8, D)
    compact = jnp.concatenate(final, 0)
    for n in range(4):
        cols = slice(n * 512, n * 512 + 512)
        wide = lax.dot_general(squeeze, compact[:, cols], tn, preferred_element_type=F32)
        outb[:, :, cols] = wide.reshape(16, 4, 512).astype(BF)

    def m5(k, c):
        dst = (ep + k) % 16
        for g in range(2):
            remote(out.at[g * 16 + dst], back.at[g * 16 + ep], m5_s.at[g], m5_r.at[g], at_ep(dst)).start()
        remote(outb.at[dst], backb.at[ep], m5_s.at[2], m5_r.at[2], at_ep(dst)).start()
        return c

    lax.fori_loop(1, 16, m5, 0)
    for g in range(2):
        back[g * 16 + ep] = out[g * 16 + ep]
    backb[ep] = outb[ep]

    relay(pm, ma, ms, TA, TB, 0)
    relay(pm, ma, ms, TA, TB, 1)

    for g in range(2):
        rep = back.at[pl.ds(g * 16, 15)]
        remote(rep, rep, m5_s.at[g], m5_r.at[g], mate).wait()
    rep = backb.at[pl.ds(0, 15)]
    remote(rep, rep, m5_s.at[2], m5_r.at[2], mate).wait()
    rw = rw_ref[...]
    share = rw / jnp.sum(rw, axis=0, keepdims=True)
    w0, w1 = column(share[0:1]), column(share[1:2])
    picks = [
        [jnp.where(c == sid_s[k][:, 0:1], 1.0, 0.0).astype(BF) for c in (slots, slotb)] for k in range(2)
    ]
    for n in range(4):
        cols = slice(n * 512, n * 512 + 512)
        rows = back[:, :, cols].reshape(256, 512)
        more = backb[:, :, cols].reshape(64, 512)
        got = [dot(pick[0], rows) + dot(pick[1], more) for pick in picks]
        oexp_ref[:, cols] = (w0 * got[0] + w1 * got[1]).astype(BF)

    for e in range(2):
        TC[1 - e].wait_recv()
        TB[e * 2].wait_recv()
        TB[e * 2 + 1].wait_recv()
        whole = pm[y, e].astype(F32) + mb[e].astype(F32) + mc[1 - e].astype(F32)
        omix_ref[e * 64:e * 64 + 64] = whole.astype(BF)

    for c in a1 + d1 + ws + X1 + XL + X2 + RC + RA + RB + TC + TA + TB + [AT]:
        c.wait_send()
    for group in (P1, P1F, P2, P2F):
        for c in group.values():
            c.wait_send()


def tables():
    freq = 1.0 / THETA ** (np.arange(ROPE // 2) * 2.0 / ROPE)
    inner = np.tile(np.arange(TOK)[:, None] * freq, (1, 4))
    first = np.tile(TOK * np.arange(128)[:, None] * freq, (1, 2))
    c, s = np.cos(first), np.sin(first)
    blocks = [[c, s], [-s, c], [s, c], [c, -s]]
    return np.stack(
        [np.cos(inner), np.sin(inner)] + [np.concatenate(b, 1) for b in blocks]
    ).astype(np.float32)


def per_device(
    query_latent, kv_latent, rope_key, query_gain, kv_gain, query_nope_w, query_rope_w,
    key_up_w, value_up_w, output_w, expert_in, moe_gain, routes, route_weight, gate_w, up_w, down_w,
):
    dma = pltpu.SemaphoreType.DMA
    vm = pl.BlockSpec(memory_space=VM)
    hbm = pl.BlockSpec(memory_space=pl.ANY)
    return pl.pallas_call(
        kernel,
        out_shape=(jax.ShapeDtypeStruct((TOK, D), BF), jax.ShapeDtypeStruct((TOK, D), BF)),
        in_specs=[vm] * 14 + [hbm] * 4,
        out_specs=(vm, vm),
        scratch_shapes=[
            VM((8, TOK, LAT), BF), VM((2, 16, KVR, 128), BF), VM((GROUP, 256), BF), VM((GROUP, 256), BF),
            VM((GROUP, 128), F32), VM((GROUP, 128), F32), VM((GROUP, 128), F32),
            VM((4, TOK, 128), BF), VM((4, TOK, 128), BF), VM((4, TOK, 128), BF),
            VM((2, 128, D), BF), VM((2, 2, D, HID), BF), VM((2, 2, D, HID), BF), VM((2, 2, HID, D), BF),
            VM((32, 8, D), BF), VM((16, 4, D), BF), VM((4, 2, 20, 8, D), BF), VM((16, 4, D), BF), VM((32, 8, D), BF),
            VM((16, 4, D), BF),
            VM((4, 2, 160, D), BF), VM((2, 160, D), BF), VM((2, 160, D), BF), VM((2, 160, D), BF), VM((2, 160, D), BF),
            VM((4, 2, 64, D), BF), VM((2, 64, D), BF), VM((2, 64, D), BF), VM((2, 64, D), BF), VM((2, 64, D), BF),
            VM((2, TOK, 128), F32), VM((TOK, D), BF),
            dma((4,)), dma((3,)), dma((3,)), dma((4,)), dma((4,)), dma((3,)), dma((3,)), dma((4,)), dma((4,)),
            dma((2, 4)), dma((2, 4)), dma((2, 4, 4)), dma((2, 4, 4)), dma((4,)), dma((4,)), dma((2,)), dma((2,)),
            dma((10,)), dma((10,)), dma((10,)), dma((10,)), dma, dma, dma((3,)), dma((3,)),
        ],
        compiler_params=pltpu.CompilerParams(
            collective_id=0, has_side_effects=True, vmem_limit_bytes=66_000_000
        ),
    )(
        query_latent, kv_latent, rope_key.T, query_gain, kv_gain.reshape(1, -1), jnp.asarray(tables()),
        query_nope_w, query_rope_w.T, key_up_w, value_up_w, expert_in, moe_gain.reshape(1, -1), routes.T, route_weight.T,
        output_w, gate_w, up_w, down_w,
    )


def solution(mesh):
    rows = P(("ep", "tp"), None)
    placed = (
        rows, rows, rows, P(), P(), P(None, "tp"), P(None, "tp"), P(None, "tp"), P(None, "tp"), P("tp", None),
        rows, P(), rows, rows, P("ep", None, "tp"), P("ep", None, "tp"), P("ep", "tp", None),
    )
    return jax.shard_map(per_device, mesh=mesh, in_specs=placed, out_specs=(rows, rows), check_vma=False)
```

```python
import functools
import math

import jax
import jax.numpy as jnp
import numpy as np
from jax import lax
from jax.experimental import pallas as pl
from jax.experimental.pallas import tpu as pltpu
from jax.sharding import PartitionSpec as P

BF = jnp.bfloat16
F32 = jnp.float32
NOPE, ROPE, VDIM = 128, 64, 128
QLAT, KVLAT, D = 768, 512, 2048
HID = 256
TOK = 128
GROUP = 1024
HALF = 512
LAT = QLAT + KVLAT + 128
KVR = HALF + HALF + HALF // 2
KVH = KVR // 2
QT = 256
THETA = 10000.0
MESH = pl.DeviceIdType.MESH
SCALE2 = math.log2(math.e) / math.sqrt(NOPE + ROPE)
VM = pltpu.VMEM


def dot(a, b):
    return jnp.dot(a, b, preferred_element_type=F32)


def kernel(
    ql_ref, kl_ref, rk_ref, qg_ref, kg_ref, tab_ref, wq_ref, wp_ref, wk_ref, wv_ref,
    xin_ref, mg_ref, routes_ref, rw_ref, ow_hbm, gw_hbm, uw_hbm, dw_hbm,
    omix_ref, oexp_ref,
    lat, kv, qa, qb, m_s, l_s, acc, att_loc, att_snd, att_rcv,
    ow, gw, uw, dw,
    out, outb, xb, bb, back, backb, pp, ra, rb, rc, sb,
    pm, ma, mb, mc, ms, sid_s, nrm,
    loc_sem, m1_s, m1_r, w_s, w_r, a1_s, a1_r, d1_s, d1_r,
    p1_s, p1_r, p2_s, p2_r, x1_s, x1_r, x2_s, x2_r,
    r_s, r_r, t_s, t_r, at_s, at_r, m5_s, m5_r,
):
    ep = lax.axis_index("ep")
    tp = lax.axis_index("tp")
    y, core = tp // 2, tp % 2
    z, x = ep // 4, ep % 4
    mate = {"ep": ep, "tp": y * 2 + 1 - core}

    def wrap(a):
        return (a + 4) % 4

    def at_y(dy):
        return {"ep": ep, "tp": wrap(y + dy) * 2 + core}

    def at_ep(e):
        return {"ep": e, "tp": tp}

    def remote(src, dst, ssem, rsem, dev):
        return pltpu.make_async_remote_copy(
            src_ref=src, dst_ref=dst, send_sem=ssem, recv_sem=rsem, device_id=dev, device_id_type=MESH
        )

    barrier = pltpu.get_barrier_semaphore()
    for dy in (1, 2, 3):
        pl.semaphore_signal(barrier, inc=1, device_id=at_y(dy), device_id_type=MESH)
    pl.semaphore_signal(barrier, inc=1, device_id=mate, device_id_type=MESH)

    def greet(k, c):
        pl.semaphore_signal(barrier, inc=1, device_id=at_ep((ep + k) % 16), device_id_type=MESH)
        return c

    lax.fori_loop(1, 16, greet, 0)

    locals_ = [
        pltpu.make_async_copy(gw_hbm, gw.at[0], loc_sem.at[0]),
        pltpu.make_async_copy(uw_hbm, uw.at[0], loc_sem.at[1]),
        pltpu.make_async_copy(dw_hbm, dw.at[0], loc_sem.at[2]),
        pltpu.make_async_copy(ow_hbm, ow.at[0], loc_sem.at[3]),
    ]
    for c in locals_:
        c.start()

    f = xin_ref[...].astype(F32)
    cen = f - jnp.mean(f, axis=-1, keepdims=True)
    var = jnp.mean(cen * cen, axis=-1, keepdims=True)
    nrm[...] = (cen * lax.rsqrt(var + 1e-05) * mg_ref[...]).astype(BF)
    rowi = lax.broadcasted_iota(jnp.int32, (TOK, TOK), 0)
    coli = lax.broadcasted_iota(jnp.int32, (TOK, TOK), 1)

    def column(row):
        return jnp.sum(jnp.where(rowi == coli, jnp.broadcast_to(row, (TOK, TOK)), 0.0), axis=1, keepdims=True)

    routes = routes_ref[...].astype(F32)
    r0, r1 = (column(routes[k:k + 1]).astype(jnp.int32) for k in range(2))
    lane = lax.broadcasted_iota(jnp.int32, (TOK, 128), 1)
    oh0 = jnp.where(lane == r0, 1.0, 0.0).astype(F32)
    oh1 = jnp.where(lane == r1, 1.0, 0.0).astype(F32)
    prior = dot(jnp.where(rowi > coli, 1.0, 0.0).astype(BF), (oh0 + oh1).astype(BF))

    def slot_of(r, oh):
        rank = jnp.sum(prior * oh, axis=1, keepdims=True)
        one = (r & 1).astype(F32)
        grp = (r >> 1).astype(F32)
        low = one * 128.0 + grp * 8.0 + rank
        high = 256.0 + grp * 4.0 + one * 2.0 + rank - 8.0
        return jnp.where(rank < 8.0, low, high)

    s0, s1 = slot_of(r0, oh0), slot_of(r1, oh1)
    sid_s[0] = jnp.broadcast_to(s0, (TOK, 128))
    sid_s[1] = jnp.broadcast_to(s1, (TOK, 128))
    slots = lax.broadcasted_iota(jnp.int32, (TOK, 256), 1).astype(F32)
    slotb = lax.broadcasted_iota(jnp.int32, (TOK, 64), 1).astype(F32) + 256.0
    sel = jnp.where((slots == s0) | (slots == s1), 1.0, 0.0).astype(BF)
    selb = jnp.where((slotb == s0) | (slotb == s1), 1.0, 0.0).astype(BF)
    tn = (((0,), (0,)), ((), ()))
    for n in range(4):
        cols = slice(n * 512, n * 512 + 512)
        got = lax.dot_general(sel, nrm[:, cols], tn, preferred_element_type=F32)
        out[:, :, cols] = got.reshape(32, 8, 512).astype(BF)
        got = lax.dot_general(selb, nrm[:, cols], tn, preferred_element_type=F32)
        outb[:, :, cols] = got.reshape(16, 4, 512).astype(BF)

    def rms(ref, gain):
        v = ref[...].astype(F32)
        sq = jnp.mean(v * v, axis=-1, keepdims=True)
        return (v * lax.rsqrt(sq + 1e-06) * gain).astype(BF)

    lat[tp, :, 0:QLAT] = rms(ql_ref, qg_ref[...].reshape(1, QLAT))
    lat[tp, :, QLAT:QLAT + KVLAT] = rms(kl_ref, kg_ref[...])
    i64 = lax.broadcasted_iota(jnp.int32, (ROPE, 128), 0)
    j64 = lax.broadcasted_iota(jnp.int32, (ROPE, 128), 1)
    plain = jnp.where(i64 == j64, 1.0, 0.0) + jnp.where(i64 + 96 == j64, 1.0, 0.0)
    turn = (plain - jnp.where(i64 + 32 == j64, jnp.where(j64 >= 64, 1.0, 0.0), 0.0)).astype(BF)

    def angles(block):
        cb, sb0 = tab_ref[0], tab_ref[1]
        k = [tab_ref[2 + n, pl.ds(block, 1), :] for n in range(4)]
        return cb * k[0] + sb0 * k[1], cb * k[2] + sb0 * k[3]

    def rotated(both, ct, st):
        return (both * ct + pltpu.roll(both, 64, 1) * st).astype(BF)

    lat[tp, :, QLAT + KVLAT:LAT] = rotated(
        lax.dot_general(rk_ref[...], turn, tn, preferred_element_type=F32), *angles(ep * 8 + tp)
    )
    wr = lax.dot_general(wp_ref[...], turn, tn, preferred_element_type=F32).astype(BF)

    pl.semaphore_wait(barrier, 19)

    def m1(k, c):
        dst = (ep + k) % 16
        for e in range(2):
            remote(out.at[e * 16 + dst], xb.at[y, e, ep], m1_s.at[e], m1_r.at[e], at_ep(dst)).start()
        remote(outb.at[dst], bb.at[ep], m1_s.at[2], m1_r.at[2], at_ep(dst)).start()
        return c

    lax.fori_loop(1, 16, m1, 0)
    for e in range(2):
        xb[y, e, ep] = out[e * 16 + ep]
    bb[ep] = outb[ep]

    a1 = [remote(lat.at[tp], lat.at[tp], a1_s.at[dy - 1], a1_r.at[dy - 1], at_y(dy)) for dy in (1, 2, 3)]
    for c in (a1[0], a1[2], a1[1]):
        c.start()
    d1 = [remote(lat.at[tp], lat.at[tp], d1_s.at[0], d1_r.at[0], mate)]
    d1[0].start()
    ws = [
        remote(gw_hbm, gw.at[1], w_s.at[0], w_r.at[0], mate),
        remote(uw_hbm, uw.at[1], w_s.at[1], w_r.at[1], mate),
        remote(dw_hbm, dw.at[1], w_s.at[2], w_r.at[2], mate),
        remote(ow_hbm, ow.at[1], w_s.at[3], w_r.at[3], mate),
    ]
    for c in ws:
        c.start()
    for dy in (1, 3, 2):
        a1[dy - 1].wait_recv()
        t = wrap(y - dy) * 2 + core
        c = remote(lat.at[t], lat.at[t], d1_s.at[dy], d1_r.at[dy], mate)
        c.start()
        d1.append(c)
    signs = (1, -1)
    for e in range(2):
        rep = xb.at[y, e, pl.ds(0, 15)]
        remote(rep, rep, m1_s.at[e], m1_r.at[e], mate).wait()
    rep = bb.at[pl.ds(0, 15)]
    remote(rep, rep, m1_s.at[2], m1_r.at[2], mate).wait()
    row64 = lax.broadcasted_iota(jnp.int32, (64, 64), 0)
    col64 = lax.broadcasted_iota(jnp.int32, (64, 64), 1)
    want = ((row64 & 31) >> 1) * 4 + (row64 >> 5) * 2 + (row64 & 1)
    squeeze = jnp.where(want == col64, 1.0, 0.0).astype(BF)
    for n in range(4):
        cols = slice(n * 512, n * 512 + 512)
        both = bb[:, :, cols].reshape(64, 512)
        tight = dot(squeeze, both).reshape(8, 8, 512).astype(BF)
        for e in range(2):
            xb[y, e, 16:20, :, cols] = tight[e * 4:e * 4 + 4]
    X1, XL, X2 = [], [], []
    for d in range(2):
        first, last = xb.at[y, d], xb.at[y, 1 - d]
        X1.append(remote(first, first, x1_s.at[d], x1_r.at[d], at_y(signs[d])))
        XL.append(remote(last, last, x1_s.at[2 + d], x1_r.at[2 + d], at_y(signs[d])))
        fw = xb.at[wrap(y - signs[d]), d]
        X2.append(remote(fw, fw, x2_s.at[d], x2_r.at[d], at_y(signs[d])))
    for c in X1:
        c.start()

    for c in d1:
        c.wait_recv()

    lane128 = lax.broadcasted_iota(jnp.int32, (HALF // 2, 128), 1)
    lane512 = lax.broadcasted_iota(jnp.int32, (HALF, 128), 1)
    for h in range(2):
        part = lat[h * 4:h * 4 + 4]
        qn = part[:, :, 0:QLAT].reshape(HALF, QLAT)
        kvn = part[:, :, QLAT:QLAT + KVLAT].reshape(HALF, KVLAT)
        rows = slice(h * HALF, h * HALF + HALF)
        qf = dot(qn, wq_ref[...])
        tabs = [angles(ep * 8 + h * 4 + t) for t in range(4)]
        rot = rotated(
            dot(qn, wr), jnp.concatenate([t[0] for t in tabs], 0), jnp.concatenate([t[1] for t in tabs], 0)
        )
        zero = jnp.zeros_like(rot)
        qa[rows, 0:128] = qf.astype(BF)
        qb[rows, 0:128] = qf.astype(BF)
        qa[rows, 128:256] = jnp.where(lane512 < 64, rot, zero)
        qb[rows, 128:256] = jnp.where(lane512 < 64, zero, rot)
        kv[h, ep, 0:HALF] = dot(kvn, wk_ref[...]).astype(BF)
        turned = jnp.transpose(dot(kvn, wv_ref[...])).astype(BF)
        for t in range(4):
            kv[h, ep, HALF + t * 128:HALF + t * 128 + 128] = turned[:, t * 128:t * 128 + 128]
        lo = part[0:2, :, QLAT + KVLAT:LAT].reshape(HALF // 2, 128)
        hi = part[2:4, :, QLAT + KVLAT:LAT].reshape(HALF // 2, 128)
        kv[h, ep, 2 * HALF:KVR] = jnp.where(lane128 < 64, lo, hi)

    def slot(h, du, dv):
        if h == 0:
            return wrap(z + dv) * 4 + wrap(x + du)
        return wrap(z + du) * 4 + wrap(x + dv)

    pieces = (slice(0, KVH), slice(KVH, KVR))
    order = (0, -1, 1, 2)
    P1, P1F, P2, P2F = {}, {}, {}, {}
    for h in range(2):
        for d in range(2):
            sg = signs[d]
            own = kv.at[h, slot(h, 0, 0)]
            P1[h, d] = remote(own, own, p1_s.at[h, d], p1_r.at[h, d], at_ep(slot(h, sg, 0)))
            fw = kv.at[h, slot(h, -sg, 0), pieces[d]]
            P1F[h, d] = remote(fw, fw, p1_s.at[h, 2 + d], p1_r.at[h, 2 + d], at_ep(slot(h, sg, 0)))
            for i in range(4):
                own = kv.at[h, slot(h, order[i], 0)]
                P2[h, i, d] = remote(own, own, p2_s.at[h, i, d], p2_r.at[h, i, d], at_ep(slot(h, 0, sg)))
                fw = kv.at[h, slot(h, order[i], -sg), pieces[d]]
                P2F[h, i, d] = remote(fw, fw, p2_s.at[h, i, 2 + d], p2_r.at[h, i, 2 + d], at_ep(slot(h, 0, sg)))

    for h in range(2):
        for d in range(2):
            P1[h, d].start()

    nt = (((1,), (1,)), ((), ()))

    def tile(qi):
        return pl.ds(qi * QT, QT)

    def scores(h, src, qi, masked):
        rots = kv[h, src, 2 * HALF:KVR]
        low = jnp.concatenate([kv[h, src, 0:256], rots], 1)
        high = jnp.concatenate([kv[h, src, 256:512], rots], 1)
        s = jnp.concatenate(
            [
                lax.dot_general(low, qa[tile(qi)], nt, preferred_element_type=F32),
                lax.dot_general(high, qb[tile(qi)], nt, preferred_element_type=F32),
            ],
            0,
        )
        if masked:
            kp = h * HALF + lax.broadcasted_iota(jnp.int32, (HALF, QT), 0)
            qp = qi * QT + lax.broadcasted_iota(jnp.int32, (HALF, QT), 1)
            s = jnp.where(kp <= qp, s, -1e30)
        return s

    def weigh(s, qi):
        old = m_s[:, tile(qi)]
        new = jnp.maximum(old, jnp.max(s, axis=0, keepdims=True))
        p = jnp.exp2((s - new[0:1]) * SCALE2)
        fac = jnp.exp2((old - new) * SCALE2)
        m_s[:, tile(qi)] = new
        l_s[:, tile(qi)] = l_s[:, tile(qi)] * fac + jnp.sum(p.reshape(HALF // 8, 8, QT), axis=0)
        return p.astype(BF), fac

    def gather_values(p, fac, h, src, qi):
        vals = jnp.concatenate([kv[h, src, HALF + t * 128:HALF + t * 128 + 128] for t in range(4)], 1)
        acc[:, tile(qi)] = acc[:, tile(qi)] * fac[0:1] + dot(vals, p)

    def run(items):
        s, prev = scores(*items[0]), None
        for n, (h, src, qi, _) in enumerate(items):
            later = scores(*items[n + 1]) if n + 1 < len(items) else None
            weighed = weigh(s, qi)
            if prev is not None:
                gather_values(*prev)
            prev, s = weighed + (h, src, qi), later
        gather_values(*prev)

    def attend_all(count, place):
        def one(n, c):
            h, du, dv = place(n)
            src = wrap(z + dv + h * (du - dv)) * 4 + wrap(x + du + h * (dv - du))

            @pl.when(src < ep)
            def _():
                run([(h, src, qi, False) for qi in range(GROUP // QT)])

            return c

        lax.fori_loop(0, count, one, 0)

    m_s[...] = jnp.full((8, GROUP), -1e30, F32)
    l_s[...] = jnp.zeros((8, GROUP), F32)
    acc[...] = jnp.zeros((VDIM, GROUP), F32)
    run([(0, ep, 0, True), (0, ep, 1, True), (0, ep, 2, False), (0, ep, 3, False), (1, ep, 2, True), (1, ep, 3, True)])

    for h in range(2):
        for d in range(2):
            P2[h, 0, d].start()
    for c in XL:
        c.start()

    def expert(ys):
        n = len(ys)

        def one(e, c):
            rows = jnp.concatenate([xb[b, e].reshape(160, D) for b in ys], 0)
            total = [None] * 4
            hid = []
            for w in range(2):
                g = jnp.minimum(dot(rows, gw[w, e]), 7.0)
                u = jnp.clip(dot(rows, uw[w, e]), -7.0, 7.0)
                hid.append((g * jax.nn.sigmoid(1.702 * g) * (u + 1.0)).astype(BF))
            both = jnp.concatenate(hid, 1)
            for q in range(4):
                cols = slice(q * 512, q * 512 + 512)
                down = jnp.concatenate([dw[0, e, :, cols], dw[1, e, :, cols]], 0)
                total = dot(both, down).astype(BF)
                for k in range(n):
                    pp[ys[k], e, :, cols] = total[k * 160:k * 160 + 160]
            return c

        lax.fori_loop(0, 2, one, 0)

    def ring(part, a_, b_, c_, s_, ssem, rsem):
        n = part.shape[2] // 2
        C, A, B = [], [], []
        for d in range(2):
            dev = at_y(signs[d])
            near = wrap(y + signs[d])
            far = wrap(y + 2)
            C.append(remote(part.at[near, 1 - d], c_.at[d], ssem.at[d], rsem.at[d], dev))
            for k in range(2):
                q = pl.ds(k * n, n)
                m = 2 + d * 2 + k
                A.append(remote(part.at[far, d, q], a_.at[d, q], ssem.at[m], rsem.at[m], dev))
                m = 6 + d * 2 + k
                B.append(remote(s_.at[d, q], b_.at[d, q], ssem.at[m], rsem.at[m], dev))
        return C, A, B

    def relay(part, a_, s_, A, B, k):
        n = part.shape[2] // 2
        q = slice(k * n, k * n + n)
        for d in range(2):
            A[d * 2 + k].wait_recv()
            s_[d, q] = (part[wrap(y + signs[d]), d, q].astype(F32) + a_[d, q].astype(F32)).astype(BF)
            B[d * 2 + k].start()

    RC, RA, RB = ring(pp, ra, rb, rc, sb, r_s, r_r)
    TC, TA, TB = ring(pm, ma, mb, mc, ms, t_s, t_r)

    def p1_on():
        for h in range(2):
            for d in range(2):
                P1[h, d].wait_recv()
                P1F[h, d].start()
        for h in range(2):
            for i in (1, 2):
                for d in range(2):
                    P2[h, i, d].start()

    def p2_on(i):
        for h in range(2):
            for d in range(2):
                P2[h, i, d].wait_recv()
                P2F[h, i, d].start()

    def p1f_on():
        for h in range(2):
            for d in range(2):
                P1F[h, d].wait_recv()
        for h in range(2):
            for d in range(2):
                P2[h, 3, d].start()

    def near(i, *halves):
        first = halves[0] if halves else 0
        attend_all(2 if halves else 4, lambda n: (first + n // 2, order[i], n % 2 * 2 - 1))

    def far(i):
        for h in range(2):
            for d in range(2):
                P2F[h, i, d].wait_recv()
        attend_all(2, lambda n: (n, order[i], 2))

    for c in locals_:
        c.wait()
    for c in ws:
        c.wait_recv()
    expert([y])
    p1_on()
    p2_on(0)
    for c in X1:
        c.wait_recv()
    for c in X2:
        c.start()
    attend_all(8, lambda n: (n // 4, (1 - n // 2 % 2) * (n % 2 * 2 - 1), n // 2 % 2 * (n % 2 * 2 - 1)))
    for c in XL:
        c.wait_recv()
    expert([wrap(y + 1), wrap(y - 1)])
    for c in RC:
        c.start()
    p1f_on()
    p2_on(1)
    p2_on(2)
    attend_all(2, lambda n: (n, 2, 0))
    near(1)
    for c in X2:
        c.wait_recv()
    expert([wrap(y + 2)])
    for k in (0, 2, 1, 3):
        RA[k].start()
    near(2)
    p2_on(3)
    near(3, 0)
    relay(pp, ra, sb, RA, RB, 0)
    near(3, 1)
    far(0)
    relay(pp, ra, sb, RA, RB, 1)
    far(1)
    far(2)

    def finish(e, k):
        if k == 0:
            RC[1 - e].wait_recv()
        RB[e * 2 + k].wait_recv()
        q = slice(k * 80, k * 80 + 80)
        return (pp[y, e, q].astype(F32) + rb[e, q].astype(F32) + rc[1 - e, q].astype(F32)).astype(BF)

    def send_back(first, count):
        def one(k, c):
            dst = first + (ep + k) % count

            @pl.when(dst != ep)
            def _():
                for g in range(2):
                    remote(out.at[g * 16 + dst], back.at[g * 16 + ep], m5_s.at[g], m5_r.at[g], at_ep(dst)).start()

            return c

        lax.fori_loop(0, count, one, 0)

    for e in range(2):
        out[e * 16:e * 16 + 10] = finish(e, 0).reshape(10, 8, D)
    send_back(0, 10)
    far(3)

    for b in range(4):
        for side, dst in ((core, att_loc), (1 - core, att_snd)):
            cols = pl.ds(pl.multiple_of((b * 2 + side) * TOK, TOK), TOK)
            total = jnp.sum(l_s[:, cols], axis=0, keepdims=True)
            dst[b] = (acc[:, cols] / total).astype(BF)
    AT = remote(att_snd, att_rcv, at_s, at_r, mate)
    AT.start()
    AT.wait_recv()
    heads = jnp.concatenate([jnp.concatenate([att_loc[b], att_rcv[b]], 0) for b in range(4)], 1)
    for q in range(4):
        cols = slice(q * 512, q * 512 + 512)
        w2 = jnp.concatenate([ow[0, :, cols], ow[1, :, cols]], 0)
        total = lax.dot_general(heads, w2, tn, preferred_element_type=F32)
        pm[:, :, :, cols] = total.astype(BF).reshape(4, 2, 64, 512)
    for c in TC:
        c.start()
    for k in (0, 2, 1, 3):
        TA[k].start()

    final = []
    for e in range(2):
        tight = finish(e, 1)
        final.append(tight[48:80])
        out[e * 16 + 10:e * 16 + 16] = tight[0:48].reshape(6, 8, D)
    send_back(10, 6)
    compact = jnp.concatenate(final, 0)
    for n in range(4):
        cols = slice(n * 512, n * 512 + 512)
        wide = lax.dot_general(squeeze, compact[:, cols], tn, preferred_element_type=F32)
        outb[:, :, cols] = wide.reshape(16, 4, 512).astype(BF)

    def last_rows(k, c):
        dst = (ep + k) % 16
        remote(outb.at[dst], backb.at[ep], m5_s.at[2], m5_r.at[2], at_ep(dst)).start()
        return c

    lax.fori_loop(1, 16, last_rows, 0)
    for g in range(2):
        back[g * 16 + ep] = out[g * 16 + ep]
    backb[ep] = outb[ep]

    relay(pm, ma, ms, TA, TB, 0)
    relay(pm, ma, ms, TA, TB, 1)

    for g in range(2):
        rep = back.at[pl.ds(g * 16, 15)]
        remote(rep, rep, m5_s.at[g], m5_r.at[g], mate).wait()
    rep = backb.at[pl.ds(0, 15)]
    remote(rep, rep, m5_s.at[2], m5_r.at[2], mate).wait()
    rw = rw_ref[...]
    share = rw / jnp.sum(rw, axis=0, keepdims=True)
    w0, w1 = column(share[0:1]), column(share[1:2])
    picks = [
        [jnp.where(c == sid_s[k][:, 0:1], 1.0, 0.0).astype(BF) for c in (slots, slotb)] for k in range(2)
    ]
    for n in range(4):
        cols = slice(n * 512, n * 512 + 512)
        rows = back[:, :, cols].reshape(256, 512)
        more = backb[:, :, cols].reshape(64, 512)
        got = [dot(pick[0], rows) + dot(pick[1], more) for pick in picks]
        oexp_ref[:, cols] = (w0 * got[0] + w1 * got[1]).astype(BF)

    for e in range(2):
        TC[1 - e].wait_recv()
        TB[e * 2].wait_recv()
        TB[e * 2 + 1].wait_recv()
        whole = pm[y, e].astype(F32) + mb[e].astype(F32) + mc[1 - e].astype(F32)
        omix_ref[e * 64:e * 64 + 64] = whole.astype(BF)

    for c in a1 + d1 + ws + X1 + XL + X2 + RC + RA + RB + TC + TA + TB + [AT]:
        c.wait_send()
    for group in (P1, P1F, P2, P2F):
        for c in group.values():
            c.wait_send()


def tables():
    freq = 1.0 / THETA ** (np.arange(ROPE // 2) * 2.0 / ROPE)
    inner = np.tile(np.arange(TOK)[:, None] * freq, (1, 4))
    first = np.tile(TOK * np.arange(128)[:, None] * freq, (1, 2))
    c, s = np.cos(first), np.sin(first)
    blocks = [[c, s], [-s, c], [s, c], [c, -s]]
    return np.stack(
        [np.cos(inner), np.sin(inner)] + [np.concatenate(b, 1) for b in blocks]
    ).astype(np.float32)


def per_device(
    query_latent, kv_latent, rope_key, query_gain, kv_gain, query_nope_w, query_rope_w,
    key_up_w, value_up_w, output_w, expert_in, moe_gain, routes, route_weight, gate_w, up_w, down_w,
):
    dma = pltpu.SemaphoreType.DMA
    vm = pl.BlockSpec(memory_space=VM)
    hbm = pl.BlockSpec(memory_space=pl.ANY)
    return pl.pallas_call(
        kernel,
        out_shape=(jax.ShapeDtypeStruct((TOK, D), BF), jax.ShapeDtypeStruct((TOK, D), BF)),
        in_specs=[vm] * 14 + [hbm] * 4,
        out_specs=(vm, vm),
        scratch_shapes=[
            VM((8, TOK, LAT), BF), VM((2, 16, KVR, 128), BF), VM((GROUP, 256), BF), VM((GROUP, 256), BF),
            VM((8, GROUP), F32), VM((8, GROUP), F32), VM((VDIM, GROUP), F32),
            VM((4, TOK, 128), BF), VM((4, TOK, 128), BF), VM((4, TOK, 128), BF),
            VM((2, 128, D), BF), VM((2, 2, D, HID), BF), VM((2, 2, D, HID), BF), VM((2, 2, HID, D), BF),
            VM((32, 8, D), BF), VM((16, 4, D), BF), VM((4, 2, 20, 8, D), BF), VM((16, 4, D), BF), VM((32, 8, D), BF),
            VM((16, 4, D), BF),
            VM((4, 2, 160, D), BF), VM((2, 160, D), BF), VM((2, 160, D), BF), VM((2, 160, D), BF), VM((2, 160, D), BF),
            VM((4, 2, 64, D), BF), VM((2, 64, D), BF), VM((2, 64, D), BF), VM((2, 64, D), BF), VM((2, 64, D), BF),
            VM((2, TOK, 128), F32), VM((TOK, D), BF),
            dma((4,)), dma((3,)), dma((3,)), dma((4,)), dma((4,)), dma((3,)), dma((3,)), dma((4,)), dma((4,)),
            dma((2, 4)), dma((2, 4)), dma((2, 4, 4)), dma((2, 4, 4)), dma((4,)), dma((4,)), dma((2,)), dma((2,)),
            dma((10,)), dma((10,)), dma((10,)), dma((10,)), dma, dma, dma((3,)), dma((3,)),
        ],
        compiler_params=pltpu.CompilerParams(
            collective_id=0, has_side_effects=True, vmem_limit_bytes=66_000_000
        ),
    )(
        query_latent, kv_latent, rope_key.T, query_gain, kv_gain.reshape(1, -1), jnp.asarray(tables()),
        query_nope_w, query_rope_w.T, key_up_w, value_up_w, expert_in, moe_gain.reshape(1, -1), routes.T, route_weight.T,
        output_w, gate_w, up_w, down_w,
    )


def solution(mesh):
    rows = P(("ep", "tp"), None)
    placed = (
        rows, rows, rows, P(), P(), P(None, "tp"), P(None, "tp"), P(None, "tp"), P(None, "tp"), P("tp", None),
        rows, P(), rows, rows, P("ep", None, "tp"), P("ep", None, "tp"), P("ep", "tp", None),
    )
    return jax.shard_map(per_device, mesh=mesh, in_specs=placed, out_specs=(rows, rows), check_vma=False)
```

```python
import functools
import math

import jax
import jax.numpy as jnp
import numpy as np
from jax import lax
from jax.experimental import pallas as pl
from jax.experimental.pallas import tpu as pltpu
from jax.sharding import PartitionSpec as P

BF = jnp.bfloat16
F32 = jnp.float32
NOPE, ROPE, VDIM = 128, 64, 128
QLAT, KVLAT, D = 768, 512, 2048
HID = 256
TOK = 128
GROUP = 1024
HALF = 512
LAT = QLAT + KVLAT + 128
KVR = HALF + HALF + HALF // 2
KVH = KVR // 2
QT = 256
THETA = 10000.0
MESH = pl.DeviceIdType.MESH
SCALE2 = math.log2(math.e) / math.sqrt(NOPE + ROPE)
VM = pltpu.VMEM


def dot(a, b):
    return jnp.dot(a, b, preferred_element_type=F32)


def kernel(
    ql_ref, kl_ref, rk_ref, qg_ref, kg_ref, tab_ref, wq_ref, wp_ref, wk_ref, wv_ref,
    xin_ref, mg_ref, routes_ref, rw_ref, ow_hbm, gw_hbm, uw_hbm, dw_hbm,
    omix_ref, oexp_ref,
    lat, kv, qa, qb, m_s, l_s, acc, att_loc, att_snd, att_rcv,
    ow, gw, uw, dw,
    out, outb, xa, xc, bb, back, backb, pp, ra, rb, rc, sb,
    pm, ma, mb, mc, ms, sid_s, nrm,
    loc_sem, m1_s, m1_r, w_s, w_r, a1_s, a1_r, d1_s, d1_r,
    p1_s, p1_r, p2_s, p2_r, x1_s, x1_r, x2_s, x2_r,
    r_s, r_r, t_s, t_r, at_s, at_r, m5_s, m5_r,
):
    ep = lax.axis_index("ep")
    tp = lax.axis_index("tp")
    y, core = tp // 2, tp % 2
    z, x = ep // 4, ep % 4
    mate = {"ep": ep, "tp": y * 2 + 1 - core}

    def wrap(a):
        return (a + 4) % 4

    def at_y(dy):
        return {"ep": ep, "tp": wrap(y + dy) * 2 + core}

    def at_ep(e):
        return {"ep": e, "tp": tp}

    def remote(src, dst, ssem, rsem, dev):
        return pltpu.make_async_remote_copy(
            src_ref=src, dst_ref=dst, send_sem=ssem, recv_sem=rsem, device_id=dev, device_id_type=MESH
        )

    barrier = pltpu.get_barrier_semaphore()
    for dy in (1, 3):
        pl.semaphore_signal(barrier, inc=1, device_id=at_y(dy), device_id_type=MESH)
    pl.semaphore_signal(barrier, inc=1, device_id=mate, device_id_type=MESH)

    def greet(k, c):
        pl.semaphore_signal(barrier, inc=1, device_id=at_ep((ep + k) % 16), device_id_type=MESH)
        return c

    lax.fori_loop(1, 16, greet, 0)

    locals_ = [
        pltpu.make_async_copy(gw_hbm, gw.at[0], loc_sem.at[0]),
        pltpu.make_async_copy(uw_hbm, uw.at[0], loc_sem.at[1]),
        pltpu.make_async_copy(dw_hbm, dw.at[0], loc_sem.at[2]),
        pltpu.make_async_copy(ow_hbm, ow.at[0], loc_sem.at[3]),
    ]
    for c in locals_:
        c.start()

    f = xin_ref[...].astype(F32)
    cen = f - jnp.mean(f, axis=-1, keepdims=True)
    var = jnp.mean(cen * cen, axis=-1, keepdims=True)
    nrm[...] = (cen * lax.rsqrt(var + 1e-05) * mg_ref[...]).astype(BF)
    rowi = lax.broadcasted_iota(jnp.int32, (TOK, TOK), 0)
    coli = lax.broadcasted_iota(jnp.int32, (TOK, TOK), 1)

    def column(row):
        return jnp.sum(jnp.where(rowi == coli, jnp.broadcast_to(row, (TOK, TOK)), 0.0), axis=1, keepdims=True)

    routes = routes_ref[...].astype(F32)
    r0, r1 = (column(routes[k:k + 1]).astype(jnp.int32) for k in range(2))
    lane = lax.broadcasted_iota(jnp.int32, (TOK, 128), 1)
    oh0 = jnp.where(lane == r0, 1.0, 0.0).astype(F32)
    oh1 = jnp.where(lane == r1, 1.0, 0.0).astype(F32)
    prior = dot(jnp.where(rowi > coli, 1.0, 0.0).astype(BF), (oh0 + oh1).astype(BF))

    def slot_of(r, oh):
        rank = jnp.sum(prior * oh, axis=1, keepdims=True)
        one = (r & 1).astype(F32)
        grp = (r >> 1).astype(F32)
        low = one * 128.0 + grp * 8.0 + rank
        high = 256.0 + grp * 4.0 + one * 2.0 + rank - 8.0
        return jnp.where(rank < 8.0, low, high)

    s0, s1 = slot_of(r0, oh0), slot_of(r1, oh1)
    sid_s[0] = jnp.broadcast_to(s0, (TOK, 128))
    sid_s[1] = jnp.broadcast_to(s1, (TOK, 128))
    slots = lax.broadcasted_iota(jnp.int32, (TOK, 256), 1).astype(F32)
    slotb = lax.broadcasted_iota(jnp.int32, (TOK, 64), 1).astype(F32) + 256.0
    sel = jnp.where((slots == s0) | (slots == s1), 1.0, 0.0).astype(BF)
    selb = jnp.where((slotb == s0) | (slotb == s1), 1.0, 0.0).astype(BF)
    tn = (((0,), (0,)), ((), ()))
    for n in range(4):
        cols = slice(n * 512, n * 512 + 512)
        got = lax.dot_general(sel, nrm[:, cols], tn, preferred_element_type=F32)
        out[:, :, cols] = got.reshape(32, 8, 512).astype(BF)
        got = lax.dot_general(selb, nrm[:, cols], tn, preferred_element_type=F32)
        outb[:, :, cols] = got.reshape(16, 4, 512).astype(BF)

    def rms(ref, gain):
        v = ref[...].astype(F32)
        sq = jnp.mean(v * v, axis=-1, keepdims=True)
        return (v * lax.rsqrt(sq + 1e-06) * gain).astype(BF)

    lat[tp, :, 0:QLAT] = rms(ql_ref, qg_ref[...].reshape(1, QLAT))
    lat[tp, :, QLAT:QLAT + KVLAT] = rms(kl_ref, kg_ref[...])
    i64 = lax.broadcasted_iota(jnp.int32, (ROPE, 128), 0)
    j64 = lax.broadcasted_iota(jnp.int32, (ROPE, 128), 1)
    plain = jnp.where(i64 == j64, 1.0, 0.0) + jnp.where(i64 + 96 == j64, 1.0, 0.0)
    turn = (plain - jnp.where(i64 + 32 == j64, jnp.where(j64 >= 64, 1.0, 0.0), 0.0)).astype(BF)

    def angles(block):
        cb, sb0 = tab_ref[0], tab_ref[1]
        k = [tab_ref[2 + n, pl.ds(block, 1), :] for n in range(4)]
        return cb * k[0] + sb0 * k[1], cb * k[2] + sb0 * k[3]

    def rotated(both, ct, st):
        return (both * ct + pltpu.roll(both, 64, 1) * st).astype(BF)

    lat[tp, :, QLAT + KVLAT:LAT] = rotated(
        lax.dot_general(rk_ref[...], turn, tn, preferred_element_type=F32), *angles(ep * 8 + tp)
    )
    wr = lax.dot_general(wp_ref[...], turn, tn, preferred_element_type=F32).astype(BF)

    pl.semaphore_wait(barrier, 18)

    signs = (1, -1)

    def m1(e):
        def one(k, c):
            dst = (ep + k) % 16
            if e < 2:
                remote(out.at[e * 16 + dst], xa.at[y, e, ep], m1_s.at[e], m1_r.at[e], at_ep(dst)).start()
            else:
                remote(outb.at[dst], bb.at[ep], m1_s.at[2], m1_r.at[2], at_ep(dst)).start()
            return c

        lax.fori_loop(1, 16, one, 0)

    m1(0)
    A1, AL, AR = [], [], []
    rowsof = (pl.ds(0, 64), pl.ds(64, 64))
    for d in range(2):
        first, last = lat.at[tp, rowsof[d]], lat.at[tp, rowsof[1 - d]]
        A1.append(remote(first, first, a1_s.at[d], a1_r.at[d], at_y(signs[d])))
        AL.append(remote(last, last, a1_s.at[2 + d], a1_r.at[2 + d], at_y(signs[d])))
        fw = lat.at[wrap(y - signs[d]) * 2 + core, rowsof[d]]
        AR.append(remote(fw, fw, a1_s.at[4 + d], a1_r.at[4 + d], at_y(signs[d])))
    for c in A1 + AL:
        c.start()
    m1(1)
    m1(2)
    d1 = []
    for dy in (0, 1, 3, 2):
        t = wrap(y - dy) * 2 + core
        d1.append(remote(lat.at[t], lat.at[t], d1_s.at[dy], d1_r.at[dy], mate))
    d1[0].start()
    ws = [
        remote(gw_hbm, gw.at[1], w_s.at[0], w_r.at[0], mate),
        remote(uw_hbm, uw.at[1], w_s.at[1], w_r.at[1], mate),
        remote(dw_hbm, dw.at[1], w_s.at[2], w_r.at[2], mate),
        remote(ow_hbm, ow.at[1], w_s.at[3], w_r.at[3], mate),
    ]
    for c in ws:
        c.start()
    for e in range(2):
        xa[y, e, ep] = out[e * 16 + ep]
    bb[ep] = outb[ep]

    XA, XC, XR, XS = [], [], [], []
    for d in range(2):
        dev = at_y(signs[d])
        XA.append([remote(xa.at[y, e], xa.at[y, e], x1_s.at[d, e], x1_r.at[d, e], dev) for e in range(2)])
        XC.append(remote(xc.at[y], xc.at[y], x1_s.at[d, 2], x1_r.at[d, 2], dev))
        b = wrap(y - signs[d])
        XR.append(remote(xa.at[b, d], xa.at[b, d], x2_s.at[d, 0], x2_r.at[d, 0], dev))
        XS.append(remote(xc.at[b, d], xc.at[b, d], x2_s.at[d, 1], x2_r.at[d, 1], dev))

    def rows_here(e):
        rep = xa.at[y, e, pl.ds(0, 15)]
        remote(rep, rep, m1_s.at[e], m1_r.at[e], mate).wait()
        for d in range(2):
            XA[d][e].start()

    for d in range(2):
        A1[d].wait_recv()
        AR[d].start()
    rows_here(0)
    for d in range(2):
        AL[d].wait_recv()
        d1[1 + d].start()
    for c in AR:
        c.wait_recv()
    d1[3].start()
    rows_here(1)
    rep = bb.at[pl.ds(0, 15)]
    remote(rep, rep, m1_s.at[2], m1_r.at[2], mate).wait()
    row64 = lax.broadcasted_iota(jnp.int32, (64, 64), 0)
    col64 = lax.broadcasted_iota(jnp.int32, (64, 64), 1)
    want = ((row64 & 31) >> 1) * 4 + (row64 >> 5) * 2 + (row64 & 1)
    squeeze = jnp.where(want == col64, 1.0, 0.0).astype(BF)
    for n in range(4):
        cols = slice(n * 512, n * 512 + 512)
        tight = dot(squeeze, bb[:, :, cols].reshape(64, 512))
        xc[y, :, :, :, cols] = tight.reshape(2, 4, 8, 512).astype(BF)
    for c in XC:
        c.start()
    for c in d1:
        c.wait_recv()

    lane128 = lax.broadcasted_iota(jnp.int32, (HALF // 2, 128), 1)
    lane512 = lax.broadcasted_iota(jnp.int32, (HALF, 128), 1)
    for h in range(2):
        part = lat[h * 4:h * 4 + 4]
        qn = part[:, :, 0:QLAT].reshape(HALF, QLAT)
        kvn = part[:, :, QLAT:QLAT + KVLAT].reshape(HALF, KVLAT)
        rows = slice(h * HALF, h * HALF + HALF)
        qf = dot(qn, wq_ref[...])
        tabs = [angles(ep * 8 + h * 4 + t) for t in range(4)]
        rot = rotated(
            dot(qn, wr), jnp.concatenate([t[0] for t in tabs], 0), jnp.concatenate([t[1] for t in tabs], 0)
        )
        zero = jnp.zeros_like(rot)
        qa[rows, 0:128] = qf.astype(BF)
        qb[rows, 0:128] = qf.astype(BF)
        qa[rows, 128:256] = jnp.where(lane512 < 64, rot, zero)
        qb[rows, 128:256] = jnp.where(lane512 < 64, zero, rot)
        kv[h, ep, 0:HALF] = dot(kvn, wk_ref[...]).astype(BF)
        turned = jnp.transpose(dot(kvn, wv_ref[...])).astype(BF)
        for t in range(4):
            kv[h, ep, HALF + t * 128:HALF + t * 128 + 128] = turned[:, t * 128:t * 128 + 128]
        lo = part[0:2, :, QLAT + KVLAT:LAT].reshape(HALF // 2, 128)
        hi = part[2:4, :, QLAT + KVLAT:LAT].reshape(HALF // 2, 128)
        kv[h, ep, 2 * HALF:KVR] = jnp.where(lane128 < 64, lo, hi)

    def slot(h, du, dv):
        if h == 0:
            return wrap(z + dv) * 4 + wrap(x + du)
        return wrap(z + du) * 4 + wrap(x + dv)

    pieces = (slice(0, KVH), slice(KVH, KVR))
    order = (0, -1, 1, 2)
    P1, P1F, P2, P2F = {}, {}, {}, {}
    for h in range(2):
        for d in range(2):
            sg = signs[d]
            own = kv.at[h, slot(h, 0, 0)]
            P1[h, d] = remote(own, own, p1_s.at[h, d], p1_r.at[h, d], at_ep(slot(h, sg, 0)))
            fw = kv.at[h, slot(h, -sg, 0), pieces[d]]
            P1F[h, d] = remote(fw, fw, p1_s.at[h, 2 + d], p1_r.at[h, 2 + d], at_ep(slot(h, sg, 0)))
            for i in range(4):
                own = kv.at[h, slot(h, order[i], 0)]
                P2[h, i, d] = remote(own, own, p2_s.at[h, i, d], p2_r.at[h, i, d], at_ep(slot(h, 0, sg)))
                fw = kv.at[h, slot(h, order[i], -sg), pieces[d]]
                P2F[h, i, d] = remote(fw, fw, p2_s.at[h, i, 2 + d], p2_r.at[h, i, 2 + d], at_ep(slot(h, 0, sg)))

    for h in range(2):
        for d in range(2):
            P1[h, d].start()

    nt = (((1,), (1,)), ((), ()))

    def tile(qi):
        return pl.ds(qi * QT, QT)

    def scores(h, src, qi, masked):
        rots = kv[h, src, 2 * HALF:KVR]
        low = jnp.concatenate([kv[h, src, 0:256], rots], 1)
        high = jnp.concatenate([kv[h, src, 256:512], rots], 1)
        s = jnp.concatenate(
            [
                lax.dot_general(low, qa[tile(qi)], nt, preferred_element_type=F32),
                lax.dot_general(high, qb[tile(qi)], nt, preferred_element_type=F32),
            ],
            0,
        )
        if masked:
            kp = h * HALF + lax.broadcasted_iota(jnp.int32, (HALF, QT), 0)
            qp = qi * QT + lax.broadcasted_iota(jnp.int32, (HALF, QT), 1)
            s = jnp.where(kp <= qp, s, -1e30)
        return s

    def weigh(s, qi):
        old = m_s[:, tile(qi)]
        new = jnp.maximum(old, jnp.max(s, axis=0, keepdims=True))
        p = jnp.exp2((s - new[0:1]) * SCALE2)
        fac = jnp.exp2((old - new) * SCALE2)
        m_s[:, tile(qi)] = new
        l_s[:, tile(qi)] = l_s[:, tile(qi)] * fac + jnp.sum(p.reshape(HALF // 8, 8, QT), axis=0)
        return p.astype(BF), fac

    def gather_values(p, fac, h, src, qi):
        vals = jnp.concatenate([kv[h, src, HALF + t * 128:HALF + t * 128 + 128] for t in range(4)], 1)
        acc[:, tile(qi)] = acc[:, tile(qi)] * fac[0:1] + dot(vals, p)

    def run(items):
        s, prev = scores(*items[0]), None
        for n, (h, src, qi, _) in enumerate(items):
            later = scores(*items[n + 1]) if n + 1 < len(items) else None
            weighed = weigh(s, qi)
            if prev is not None:
                gather_values(*prev)
            prev, s = weighed + (h, src, qi), later
        gather_values(*prev)

    def attend_all(count, place):
        def one(n, c):
            h, du, dv = place(n)
            src = wrap(z + dv + h * (du - dv)) * 4 + wrap(x + du + h * (dv - du))

            @pl.when(src < ep)
            def _():
                run([(h, src, qi, False) for qi in range(GROUP // QT)])

            return c

        lax.fori_loop(0, count, one, 0)

    m_s[...] = jnp.full((8, GROUP), -1e30, F32)
    l_s[...] = jnp.zeros((8, GROUP), F32)
    acc[...] = jnp.zeros((VDIM, GROUP), F32)
    run([(0, ep, 0, True), (0, ep, 1, True), (0, ep, 2, False), (0, ep, 3, False), (1, ep, 2, True), (1, ep, 3, True)])

    for h in range(2):
        for d in range(2):
            P2[h, 0, d].start()

    def expert(ys):
        n = len(ys)

        def one(e, c):
            rows = jnp.concatenate([r for b in ys for r in (xa[b, e].reshape(128, D), xc[b, e].reshape(32, D))], 0)
            total = [None] * 4
            hid = []
            for w in range(2):
                g = jnp.minimum(dot(rows, gw[w, e]), 7.0)
                u = jnp.clip(dot(rows, uw[w, e]), -7.0, 7.0)
                hid.append((g * jax.nn.sigmoid(1.702 * g) * (u + 1.0)).astype(BF))
            both = jnp.concatenate(hid, 1)
            for q in range(4):
                cols = slice(q * 512, q * 512 + 512)
                down = jnp.concatenate([dw[0, e, :, cols], dw[1, e, :, cols]], 0)
                total = dot(both, down).astype(BF)
                for k in range(n):
                    pp[ys[k], e, :, cols] = total[k * 160:k * 160 + 160]
            return c

        lax.fori_loop(0, 2, one, 0)

    def ring(part, a_, b_, c_, s_, ssem, rsem):
        n = part.shape[2] // 2
        C, A, B = [], [], []
        for d in range(2):
            dev = at_y(signs[d])
            near = wrap(y + signs[d])
            far = wrap(y + 2)
            C.append(remote(part.at[near, 1 - d], c_.at[d], ssem.at[d], rsem.at[d], dev))
            for k in range(2):
                q = pl.ds(k * n, n)
                m = 2 + d * 2 + k
                A.append(remote(part.at[far, d, q], a_.at[d, q], ssem.at[m], rsem.at[m], dev))
                m = 6 + d * 2 + k
                B.append(remote(s_.at[d, q], b_.at[d, q], ssem.at[m], rsem.at[m], dev))
        return C, A, B

    def relay(part, a_, s_, A, B, k):
        n = part.shape[2] // 2
        q = slice(k * n, k * n + n)
        for d in range(2):
            A[d * 2 + k].wait_recv()
            s_[d, q] = (part[wrap(y + signs[d]), d, q].astype(F32) + a_[d, q].astype(F32)).astype(BF)
            B[d * 2 + k].start()

    RC, RA, RB = ring(pp, ra, rb, rc, sb, r_s, r_r)
    TC, TA, TB = ring(pm, ma, mb, mc, ms, t_s, t_r)

    def p1_on():
        for h in range(2):
            for d in range(2):
                P1[h, d].wait_recv()
                P1F[h, d].start()
        for h in range(2):
            for i in (1, 2):
                for d in range(2):
                    P2[h, i, d].start()

    def p2_on(i):
        for h in range(2):
            for d in range(2):
                P2[h, i, d].wait_recv()
                P2F[h, i, d].start()

    def p1f_on():
        for h in range(2):
            for d in range(2):
                P1F[h, d].wait_recv()
        for h in range(2):
            for d in range(2):
                P2[h, 3, d].start()

    def near(i, *halves):
        first = halves[0] if halves else 0
        attend_all(2 if halves else 4, lambda n: (first + n // 2, order[i], n % 2 * 2 - 1))

    def far(i):
        for h in range(2):
            for d in range(2):
                P2F[h, i, d].wait_recv()
        attend_all(2, lambda n: (n, order[i], 2))

    for c in locals_:
        c.wait()
    for c in ws:
        c.wait_recv()
    expert([y])
    XA[0][0].wait_recv()
    XR[0].start()
    p1_on()
    p2_on(0)
    XA[1][1].wait_recv()
    XR[1].start()
    attend_all(8, lambda n: (n // 4, (1 - n // 2 % 2) * (n % 2 * 2 - 1), n // 2 % 2 * (n % 2 * 2 - 1)))
    for d in range(2):
        XC[d].wait_recv()
        XS[d].start()
    XA[0][1].wait_recv()
    XA[1][0].wait_recv()
    expert([wrap(y + 1), wrap(y - 1)])
    for c in RC:
        c.start()
    p1f_on()
    p2_on(1)
    p2_on(2)
    attend_all(2, lambda n: (n, 2, 0))
    near(1)
    for c in XR + XS:
        c.wait_recv()
    expert([wrap(y + 2)])
    for k in (0, 2, 1, 3):
        RA[k].start()
    near(2)
    p2_on(3)
    near(3, 0)
    relay(pp, ra, sb, RA, RB, 0)
    near(3, 1)
    far(0)
    relay(pp, ra, sb, RA, RB, 1)
    far(1)
    far(2)

    def finish(e, k):
        if k == 0:
            RC[1 - e].wait_recv()
        RB[e * 2 + k].wait_recv()
        q = slice(k * 80, k * 80 + 80)
        return (pp[y, e, q].astype(F32) + rb[e, q].astype(F32) + rc[1 - e, q].astype(F32)).astype(BF)

    def send_back(first, count):
        def one(k, c):
            dst = first + (ep + k) % count

            @pl.when(dst != ep)
            def _():
                for g in range(2):
                    remote(out.at[g * 16 + dst], back.at[g * 16 + ep], m5_s.at[g], m5_r.at[g], at_ep(dst)).start()

            return c

        lax.fori_loop(0, count, one, 0)

    for e in range(2):
        out[e * 16:e * 16 + 10] = finish(e, 0).reshape(10, 8, D)
    send_back(0, 10)
    far(3)

    for b in range(4):
        for side, dst in ((core, att_loc), (1 - core, att_snd)):
            cols = pl.ds(pl.multiple_of((b * 2 + side) * TOK, TOK), TOK)
            total = jnp.sum(l_s[:, cols], axis=0, keepdims=True)
            dst[b] = (acc[:, cols] / total).astype(BF)
    AT = remote(att_snd, att_rcv, at_s, at_r, mate)
    AT.start()
    AT.wait_recv()
    heads = jnp.concatenate([jnp.concatenate([att_loc[b], att_rcv[b]], 0) for b in range(4)], 1)
    for q in range(4):
        cols = slice(q * 512, q * 512 + 512)
        w2 = jnp.concatenate([ow[0, :, cols], ow[1, :, cols]], 0)
        total = lax.dot_general(heads, w2, tn, preferred_element_type=F32)
        pm[:, :, :, cols] = total.astype(BF).reshape(4, 2, 64, 512)
    for c in TC:
        c.start()
    for k in (0, 2, 1, 3):
        TA[k].start()

    final = []
    for e in range(2):
        tight = finish(e, 1)
        final.append(tight[48:80])
        out[e * 16 + 10:e * 16 + 16] = tight[0:48].reshape(6, 8, D)
    send_back(10, 6)
    compact = jnp.concatenate(final, 0)
    for n in range(4):
        cols = slice(n * 512, n * 512 + 512)
        wide = lax.dot_general(squeeze, compact[:, cols], tn, preferred_element_type=F32)
        outb[:, :, cols] = wide.reshape(16, 4, 512).astype(BF)

    def last_rows(k, c):
        dst = (ep + k) % 16
        remote(outb.at[dst], backb.at[ep], m5_s.at[2], m5_r.at[2], at_ep(dst)).start()
        return c

    lax.fori_loop(1, 16, last_rows, 0)
    for g in range(2):
        back[g * 16 + ep] = out[g * 16 + ep]
    backb[ep] = outb[ep]

    relay(pm, ma, ms, TA, TB, 0)
    relay(pm, ma, ms, TA, TB, 1)

    for g in range(2):
        rep = back.at[pl.ds(g * 16, 15)]
        remote(rep, rep, m5_s.at[g], m5_r.at[g], mate).wait()
    rep = backb.at[pl.ds(0, 15)]
    remote(rep, rep, m5_s.at[2], m5_r.at[2], mate).wait()
    rw = rw_ref[...]
    share = rw / jnp.sum(rw, axis=0, keepdims=True)
    w0, w1 = column(share[0:1]), column(share[1:2])
    picks = [
        [jnp.where(c == sid_s[k][:, 0:1], 1.0, 0.0).astype(BF) for c in (slots, slotb)] for k in range(2)
    ]
    for n in range(4):
        cols = slice(n * 512, n * 512 + 512)
        rows = back[:, :, cols].reshape(256, 512)
        more = backb[:, :, cols].reshape(64, 512)
        got = [dot(pick[0], rows) + dot(pick[1], more) for pick in picks]
        oexp_ref[:, cols] = (w0 * got[0] + w1 * got[1]).astype(BF)

    for e in range(2):
        TC[1 - e].wait_recv()
        TB[e * 2].wait_recv()
        TB[e * 2 + 1].wait_recv()
        whole = pm[y, e].astype(F32) + mb[e].astype(F32) + mc[1 - e].astype(F32)
        omix_ref[e * 64:e * 64 + 64] = whole.astype(BF)

    for c in A1 + AL + AR + d1 + ws + XA[0] + XA[1] + XC + XR + XS + RC + RA + RB + TC + TA + TB + [AT]:
        c.wait_send()
    for group in (P1, P1F, P2, P2F):
        for c in group.values():
            c.wait_send()


def tables():
    freq = 1.0 / THETA ** (np.arange(ROPE // 2) * 2.0 / ROPE)
    inner = np.tile(np.arange(TOK)[:, None] * freq, (1, 4))
    first = np.tile(TOK * np.arange(128)[:, None] * freq, (1, 2))
    c, s = np.cos(first), np.sin(first)
    blocks = [[c, s], [-s, c], [s, c], [c, -s]]
    return np.stack(
        [np.cos(inner), np.sin(inner)] + [np.concatenate(b, 1) for b in blocks]
    ).astype(np.float32)


def per_device(
    query_latent, kv_latent, rope_key, query_gain, kv_gain, query_nope_w, query_rope_w,
    key_up_w, value_up_w, output_w, expert_in, moe_gain, routes, route_weight, gate_w, up_w, down_w,
):
    dma = pltpu.SemaphoreType.DMA
    vm = pl.BlockSpec(memory_space=VM)
    hbm = pl.BlockSpec(memory_space=pl.ANY)
    return pl.pallas_call(
        kernel,
        out_shape=(jax.ShapeDtypeStruct((TOK, D), BF), jax.ShapeDtypeStruct((TOK, D), BF)),
        in_specs=[vm] * 14 + [hbm] * 4,
        out_specs=(vm, vm),
        scratch_shapes=[
            VM((8, TOK, LAT), BF), VM((2, 16, KVR, 128), BF), VM((GROUP, 256), BF), VM((GROUP, 256), BF),
            VM((8, GROUP), F32), VM((8, GROUP), F32), VM((VDIM, GROUP), F32),
            VM((4, TOK, 128), BF), VM((4, TOK, 128), BF), VM((4, TOK, 128), BF),
            VM((2, 128, D), BF), VM((2, 2, D, HID), BF), VM((2, 2, D, HID), BF), VM((2, 2, HID, D), BF),
            VM((32, 8, D), BF), VM((16, 4, D), BF), VM((4, 2, 16, 8, D), BF), VM((4, 2, 4, 8, D), BF), VM((16, 4, D), BF), VM((32, 8, D), BF),
            VM((16, 4, D), BF),
            VM((4, 2, 160, D), BF), VM((2, 160, D), BF), VM((2, 160, D), BF), VM((2, 160, D), BF), VM((2, 160, D), BF),
            VM((4, 2, 64, D), BF), VM((2, 64, D), BF), VM((2, 64, D), BF), VM((2, 64, D), BF), VM((2, 64, D), BF),
            VM((2, TOK, 128), F32), VM((TOK, D), BF),
            dma((4,)), dma((3,)), dma((3,)), dma((4,)), dma((4,)), dma((6,)), dma((6,)), dma((4,)), dma((4,)),
            dma((2, 4)), dma((2, 4)), dma((2, 4, 4)), dma((2, 4, 4)), dma((2, 3)), dma((2, 3)), dma((2, 2)), dma((2, 2)),
            dma((10,)), dma((10,)), dma((10,)), dma((10,)), dma, dma, dma((3,)), dma((3,)),
        ],
        compiler_params=pltpu.CompilerParams(
            collective_id=0, has_side_effects=True, vmem_limit_bytes=66_000_000
        ),
    )(
        query_latent, kv_latent, rope_key.T, query_gain, kv_gain.reshape(1, -1), jnp.asarray(tables()),
        query_nope_w, query_rope_w.T, key_up_w, value_up_w, expert_in, moe_gain.reshape(1, -1), routes.T, route_weight.T,
        output_w, gate_w, up_w, down_w,
    )


def solution(mesh):
    rows = P(("ep", "tp"), None)
    placed = (
        rows, rows, rows, P(), P(), P(None, "tp"), P(None, "tp"), P(None, "tp"), P(None, "tp"), P("tp", None),
        rows, P(), rows, rows, P("ep", None, "tp"), P("ep", None, "tp"), P("ep", "tp", None),
    )
    return jax.shard_map(per_device, mesh=mesh, in_specs=placed, out_specs=(rows, rows), check_vma=False)
```

```python
import functools
import math

import jax
import jax.numpy as jnp
import numpy as np
from jax import lax
from jax.experimental import pallas as pl
from jax.experimental.pallas import tpu as pltpu
from jax.sharding import PartitionSpec as P

BF = jnp.bfloat16
F32 = jnp.float32
NOPE, ROPE, VDIM = 128, 64, 128
QLAT, KVLAT, D = 768, 512, 2048
HID = 256
TOK = 128
GROUP = 1024
HALF = 512
LAT = QLAT + KVLAT + 128
KVR = HALF + HALF + HALF // 2
KVH = KVR // 2
QT = 256
THETA = 10000.0
MESH = pl.DeviceIdType.MESH
SCALE2 = math.log2(math.e) / math.sqrt(NOPE + ROPE)
VM = pltpu.VMEM


def dot(a, b):
    return jnp.dot(a, b, preferred_element_type=F32)


def kernel(
    ql_ref, kl_ref, rk_ref, qg_ref, kg_ref, tab_ref, wq_ref, wp_ref, wk_ref, wv_ref,
    xin_ref, mg_ref, routes_ref, rw_ref, ow_hbm, gw_hbm, uw_hbm, dw_hbm,
    omix_ref, oexp_ref,
    lat, kv, qa, qb, m_s, l_s, acc, att_loc, att_snd, att_rcv,
    wall, hl, hr, gw, uw, dw,
    out, outb, xa, xc, bb, back, backb, pp, ra, rb, rc, sb,
    sid_s, nrm,
    loc_sem, m1_s, m1_r, w_s, w_r, a1_s, a1_r, d1_s, d1_r,
    p1_s, p1_r, p2_s, p2_r, x1_s, x1_r, x2_s, x2_r,
    r_s, r_r, o1_s, o1_r, o2_s, o2_r, o4_s, o4_r, o3_s, o3_r, h_s, h_r, at_s, at_r, m5_s, m5_r,
):
    ep = lax.axis_index("ep")
    tp = lax.axis_index("tp")
    y, core = tp // 2, tp % 2
    z, x = ep // 4, ep % 4
    mate = {"ep": ep, "tp": y * 2 + 1 - core}

    def wrap(a):
        return (a + 4) % 4

    def at_y(dy):
        return {"ep": ep, "tp": wrap(y + dy) * 2 + core}

    def at_ep(e):
        return {"ep": e, "tp": tp}

    def remote(src, dst, ssem, rsem, dev):
        return pltpu.make_async_remote_copy(
            src_ref=src, dst_ref=dst, send_sem=ssem, recv_sem=rsem, device_id=dev, device_id_type=MESH
        )

    barrier = pltpu.get_barrier_semaphore()
    for dy in (1, 2, 3):
        pl.semaphore_signal(barrier, inc=1, device_id=at_y(dy), device_id_type=MESH)
    pl.semaphore_signal(barrier, inc=1, device_id=mate, device_id_type=MESH)

    def greet(k, c):
        pl.semaphore_signal(barrier, inc=1, device_id=at_ep((ep + k) % 16), device_id_type=MESH)
        return c

    lax.fori_loop(1, 16, greet, 0)

    locals_ = [
        pltpu.make_async_copy(gw_hbm, gw.at[0], loc_sem.at[0]),
        pltpu.make_async_copy(uw_hbm, uw.at[0], loc_sem.at[1]),
        pltpu.make_async_copy(dw_hbm, dw.at[0], loc_sem.at[2]),
        pltpu.make_async_copy(ow_hbm, wall.at[y, core], loc_sem.at[3]),
    ]
    for c in locals_:
        c.start()

    f = xin_ref[...].astype(F32)
    cen = f - jnp.mean(f, axis=-1, keepdims=True)
    var = jnp.mean(cen * cen, axis=-1, keepdims=True)
    nrm[...] = (cen * lax.rsqrt(var + 1e-05) * mg_ref[...]).astype(BF)
    rowi = lax.broadcasted_iota(jnp.int32, (TOK, TOK), 0)
    coli = lax.broadcasted_iota(jnp.int32, (TOK, TOK), 1)

    def column(row):
        return jnp.sum(jnp.where(rowi == coli, jnp.broadcast_to(row, (TOK, TOK)), 0.0), axis=1, keepdims=True)

    routes = routes_ref[...].astype(F32)
    r0, r1 = (column(routes[k:k + 1]).astype(jnp.int32) for k in range(2))
    lane = lax.broadcasted_iota(jnp.int32, (TOK, 128), 1)
    oh0 = jnp.where(lane == r0, 1.0, 0.0).astype(F32)
    oh1 = jnp.where(lane == r1, 1.0, 0.0).astype(F32)
    prior = dot(jnp.where(rowi > coli, 1.0, 0.0).astype(BF), (oh0 + oh1).astype(BF))

    def slot_of(r, oh):
        rank = jnp.sum(prior * oh, axis=1, keepdims=True)
        one = (r & 1).astype(F32)
        grp = (r >> 1).astype(F32)
        low = one * 128.0 + grp * 8.0 + rank
        high = 256.0 + grp * 4.0 + one * 2.0 + rank - 8.0
        return jnp.where(rank < 8.0, low, high)

    s0, s1 = slot_of(r0, oh0), slot_of(r1, oh1)
    sid_s[0] = jnp.broadcast_to(s0, (TOK, 128))
    sid_s[1] = jnp.broadcast_to(s1, (TOK, 128))
    slots = lax.broadcasted_iota(jnp.int32, (TOK, 256), 1).astype(F32)
    slotb = lax.broadcasted_iota(jnp.int32, (TOK, 64), 1).astype(F32) + 256.0
    sel = jnp.where((slots == s0) | (slots == s1), 1.0, 0.0).astype(BF)
    selb = jnp.where((slotb == s0) | (slotb == s1), 1.0, 0.0).astype(BF)
    tn = (((0,), (0,)), ((), ()))
    for n in range(4):
        cols = slice(n * 512, n * 512 + 512)
        got = lax.dot_general(sel, nrm[:, cols], tn, preferred_element_type=F32)
        out[:, :, cols] = got.reshape(32, 8, 512).astype(BF)
        got = lax.dot_general(selb, nrm[:, cols], tn, preferred_element_type=F32)
        outb[:, :, cols] = got.reshape(16, 4, 512).astype(BF)

    def rms(ref, gain):
        v = ref[...].astype(F32)
        sq = jnp.mean(v * v, axis=-1, keepdims=True)
        return (v * lax.rsqrt(sq + 1e-06) * gain).astype(BF)

    lat[tp, :, 0:QLAT] = rms(ql_ref, qg_ref[...].reshape(1, QLAT))
    lat[tp, :, QLAT:QLAT + KVLAT] = rms(kl_ref, kg_ref[...])
    i64 = lax.broadcasted_iota(jnp.int32, (ROPE, 128), 0)
    j64 = lax.broadcasted_iota(jnp.int32, (ROPE, 128), 1)
    plain = jnp.where(i64 == j64, 1.0, 0.0) + jnp.where(i64 + 96 == j64, 1.0, 0.0)
    turn = (plain - jnp.where(i64 + 32 == j64, jnp.where(j64 >= 64, 1.0, 0.0), 0.0)).astype(BF)

    def angles(block):
        cb, sb0 = tab_ref[0], tab_ref[1]
        k = [tab_ref[2 + n, pl.ds(block, 1), :] for n in range(4)]
        return cb * k[0] + sb0 * k[1], cb * k[2] + sb0 * k[3]

    def rotated(both, ct, st):
        return (both * ct + pltpu.roll(both, 64, 1) * st).astype(BF)

    lat[tp, :, QLAT + KVLAT:LAT] = rotated(
        lax.dot_general(rk_ref[...], turn, tn, preferred_element_type=F32), *angles(ep * 8 + tp)
    )
    wr = lax.dot_general(wp_ref[...], turn, tn, preferred_element_type=F32).astype(BF)

    pl.semaphore_wait(barrier, 19)

    signs = (1, -1)
    place = ep * 13 % 16

    def m1(e):
        def one(k, c):
            dst = (ep + k) % 16
            if e < 2:
                remote(out.at[e * 16 + dst], xa.at[y, e, place], m1_s.at[e], m1_r.at[e], at_ep(dst)).start()
            else:
                remote(outb.at[dst], bb.at[ep], m1_s.at[2], m1_r.at[2], at_ep(dst)).start()
            return c

        lax.fori_loop(1, 16, one, 0)

    m1(0)
    A1, AL, AR = [], [], []
    rowsof = (pl.ds(0, 64), pl.ds(64, 64))
    for d in range(2):
        first, last = lat.at[tp, rowsof[d]], lat.at[tp, rowsof[1 - d]]
        A1.append(remote(first, first, a1_s.at[d], a1_r.at[d], at_y(signs[d])))
        AL.append(remote(last, last, a1_s.at[2 + d], a1_r.at[2 + d], at_y(signs[d])))
        fw = lat.at[wrap(y - signs[d]) * 2 + core, rowsof[d]]
        AR.append(remote(fw, fw, a1_s.at[4 + d], a1_r.at[4 + d], at_y(signs[d])))
    for c in A1 + AL:
        c.start()
    m1(1)
    m1(2)
    d1 = []
    for dy in (0, 1, 3, 2):
        t = wrap(y - dy) * 2 + core
        d1.append(remote(lat.at[t], lat.at[t], d1_s.at[dy], d1_r.at[dy], mate))
    d1[0].start()
    ws = [
        remote(gw_hbm, gw.at[1], w_s.at[0], w_r.at[0], mate),
        remote(uw_hbm, uw.at[1], w_s.at[1], w_r.at[1], mate),
        remote(dw_hbm, dw.at[1], w_s.at[2], w_r.at[2], mate),
        remote(ow_hbm, wall.at[y, core], w_s.at[3], w_r.at[3], mate),
    ]
    for c in ws:
        c.start()
    OP, WD = [], []
    for dy in range(1, 4):
        OP.append(remote(ow_hbm.at[ep], wall.at[y, core, ep], o1_s.at[dy - 1], o1_r.at[dy - 1], at_y(dy)))
        b = wall.at[wrap(y - dy), core]
        WD.append(remote(b, b, o3_s.at[dy - 1], o3_r.at[dy - 1], mate))
    for c in OP:
        c.start()

    for e in range(2):
        xa[y, e, place] = out[e * 16 + ep]
    bb[ep] = outb[ep]

    XA, XC, XR, XS = [], [], [], []
    for d in range(2):
        dev = at_y(signs[d])
        XA.append([remote(xa.at[y, e], xa.at[y, e], x1_s.at[d, e], x1_r.at[d, e], dev) for e in range(2)])
        XC.append(remote(xc.at[y], xc.at[y], x1_s.at[d, 2], x1_r.at[d, 2], dev))
        b = wrap(y - signs[d])
        XR.append(remote(xa.at[b, d], xa.at[b, d], x2_s.at[d, 0], x2_r.at[d, 0], dev))
        XS.append(remote(xc.at[b, d], xc.at[b, d], x2_s.at[d, 1], x2_r.at[d, 1], dev))

    def rows_here(e):
        rep = xa.at[y, e, pl.ds(0, 15)]
        remote(rep, rep, m1_s.at[e], m1_r.at[e], mate).wait()
        for d in range(2):
            XA[d][e].start()

    for d in range(2):
        A1[d].wait_recv()
        AR[d].start()
    rows_here(0)
    for d in range(2):
        AL[d].wait_recv()
        d1[1 + d].start()
    for c in AR:
        c.wait_recv()
    d1[3].start()
    rows_here(1)
    rep = bb.at[pl.ds(0, 15)]
    remote(rep, rep, m1_s.at[2], m1_r.at[2], mate).wait()
    row64 = lax.broadcasted_iota(jnp.int32, (64, 64), 0)
    col64 = lax.broadcasted_iota(jnp.int32, (64, 64), 1)
    want = ((row64 & 31) >> 1) * 4 + (row64 >> 5) * 2 + (row64 & 1)
    squeeze = jnp.where(want == col64, 1.0, 0.0).astype(BF)
    for n in range(4):
        cols = slice(n * 512, n * 512 + 512)
        tight = dot(squeeze, bb[:, :, cols].reshape(64, 512))
        xc[y, :, :, :, cols] = tight.reshape(2, 4, 8, 512).astype(BF)
    for c in XC:
        c.start()
    for c in d1:
        c.wait_recv()

    lane128 = lax.broadcasted_iota(jnp.int32, (HALF // 2, 128), 1)
    lane512 = lax.broadcasted_iota(jnp.int32, (HALF, 128), 1)
    for h in range(2):
        part = lat[h * 4:h * 4 + 4]
        qn = part[:, :, 0:QLAT].reshape(HALF, QLAT)
        kvn = part[:, :, QLAT:QLAT + KVLAT].reshape(HALF, KVLAT)
        rows = slice(h * HALF, h * HALF + HALF)
        qf = dot(qn, wq_ref[...])
        tabs = [angles(ep * 8 + h * 4 + t) for t in range(4)]
        rot = rotated(
            dot(qn, wr), jnp.concatenate([t[0] for t in tabs], 0), jnp.concatenate([t[1] for t in tabs], 0)
        )
        zero = jnp.zeros_like(rot)
        qa[rows, 0:128] = qf.astype(BF)
        qb[rows, 0:128] = qf.astype(BF)
        qa[rows, 128:256] = jnp.where(lane512 < 64, rot, zero)
        qb[rows, 128:256] = jnp.where(lane512 < 64, zero, rot)
        kv[h, ep, 0:HALF] = dot(kvn, wk_ref[...]).astype(BF)
        turned = jnp.transpose(dot(kvn, wv_ref[...])).astype(BF)
        for t in range(4):
            kv[h, ep, HALF + t * 128:HALF + t * 128 + 128] = turned[:, t * 128:t * 128 + 128]
        lo = part[0:2, :, QLAT + KVLAT:LAT].reshape(HALF // 2, 128)
        hi = part[2:4, :, QLAT + KVLAT:LAT].reshape(HALF // 2, 128)
        kv[h, ep, 2 * HALF:KVR] = jnp.where(lane128 < 64, lo, hi)

    def slot(h, du, dv):
        if h == 0:
            return wrap(z + dv) * 4 + wrap(x + du)
        return wrap(z + du) * 4 + wrap(x + dv)

    pieces = (slice(0, KVH), slice(KVH, KVR))
    order = (0, -1, 1, 2)
    P1, P1F, P2, P2F = {}, {}, {}, {}
    for h in range(2):
        for d in range(2):
            sg = signs[d]
            own = kv.at[h, slot(h, 0, 0)]
            P1[h, d] = remote(own, own, p1_s.at[h, d], p1_r.at[h, d], at_ep(slot(h, sg, 0)))
            fw = kv.at[h, slot(h, -sg, 0), pieces[d]]
            P1F[h, d] = remote(fw, fw, p1_s.at[h, 2 + d], p1_r.at[h, 2 + d], at_ep(slot(h, sg, 0)))
            for i in range(4):
                own = kv.at[h, slot(h, order[i], 0)]
                P2[h, i, d] = remote(own, own, p2_s.at[h, i, d], p2_r.at[h, i, d], at_ep(slot(h, 0, sg)))
                fw = kv.at[h, slot(h, order[i], -sg), pieces[d]]
                P2F[h, i, d] = remote(fw, fw, p2_s.at[h, i, 2 + d], p2_r.at[h, i, 2 + d], at_ep(slot(h, 0, sg)))

    for h in range(2):
        for d in range(2):
            P1[h, d].start()

    nt = (((1,), (1,)), ((), ()))

    def tile(qi):
        return pl.ds(qi * QT, QT)

    def scores(h, src, qi, masked):
        rots = kv[h, src, 2 * HALF:KVR]
        low = jnp.concatenate([kv[h, src, 0:256], rots], 1)
        high = jnp.concatenate([kv[h, src, 256:512], rots], 1)
        s = jnp.concatenate(
            [
                lax.dot_general(low, qa[tile(qi)], nt, preferred_element_type=F32),
                lax.dot_general(high, qb[tile(qi)], nt, preferred_element_type=F32),
            ],
            0,
        )
        if masked:
            kp = h * HALF + lax.broadcasted_iota(jnp.int32, (HALF, QT), 0)
            qp = qi * QT + lax.broadcasted_iota(jnp.int32, (HALF, QT), 1)
            s = jnp.where(kp <= qp, s, -1e30)
        return s

    def weigh(s, qi):
        old = m_s[:, tile(qi)]
        new = jnp.maximum(old, jnp.max(s, axis=0, keepdims=True))
        p = jnp.exp2((s - new[0:1]) * SCALE2)
        fac = jnp.exp2((old - new) * SCALE2)
        m_s[:, tile(qi)] = new
        l_s[:, tile(qi)] = l_s[:, tile(qi)] * fac + jnp.sum(p.reshape(HALF // 8, 8, QT), axis=0)
        return p.astype(BF), fac

    def gather_values(p, fac, h, src, qi):
        vals = jnp.concatenate([kv[h, src, HALF + t * 128:HALF + t * 128 + 128] for t in range(4)], 1)
        acc[:, tile(qi)] = acc[:, tile(qi)] * fac[0:1] + dot(vals, p)

    def run(items):
        s, prev = scores(*items[0]), None
        for n, (h, src, qi, _) in enumerate(items):
            later = scores(*items[n + 1]) if n + 1 < len(items) else None
            weighed = weigh(s, qi)
            if prev is not None:
                gather_values(*prev)
            prev, s = weighed + (h, src, qi), later
        gather_values(*prev)

    def attend_all(count, place):
        def one(n, c):
            h, du, dv = place(n)
            src = wrap(z + dv + h * (du - dv)) * 4 + wrap(x + du + h * (dv - du))

            @pl.when(src < ep)
            def _():
                run([(h, src, qi, False) for qi in range(GROUP // QT)])

            return c

        lax.fori_loop(0, count, one, 0)

    m_s[...] = jnp.full((8, GROUP), -1e30, F32)
    l_s[...] = jnp.zeros((8, GROUP), F32)
    acc[...] = jnp.zeros((VDIM, GROUP), F32)
    run([(0, ep, 0, True), (0, ep, 1, True), (0, ep, 2, False), (0, ep, 3, False), (1, ep, 2, True), (1, ep, 3, True)])

    for h in range(2):
        for d in range(2):
            P2[h, 0, d].start()

    def expert(ys):
        n = len(ys)

        def one(e, c):
            rows = jnp.concatenate([r for b in ys for r in (xc[b, e].reshape(32, D), xa[b, e].reshape(128, D))], 0)
            total = [None] * 4
            hid = []
            for w in range(2):
                g = jnp.minimum(dot(rows, gw[w, e]), 7.0)
                u = jnp.clip(dot(rows, uw[w, e]), -7.0, 7.0)
                hid.append((g * jax.nn.sigmoid(1.702 * g) * (u + 1.0)).astype(BF))
            both = jnp.concatenate(hid, 1)
            for q in range(4):
                cols = slice(q * 512, q * 512 + 512)
                down = jnp.concatenate([dw[0, e, :, cols], dw[1, e, :, cols]], 0)
                total = dot(both, down).astype(BF)
                for k in range(n):
                    pp[ys[k], e, :, cols] = total[k * 160:k * 160 + 160]
            return c

        lax.fori_loop(0, 2, one, 0)

    def ring(part, a_, b_, c_, s_, ssem, rsem, cuts):
        C, A, B = [], [], []
        m = 0
        for d in range(2):
            dev = at_y(signs[d])
            near_y = wrap(y + signs[d])
            for lo, hi in cuts:
                q = pl.ds(lo, hi - lo)
                A.append(remote(part.at[wrap(y + 2), d, q], a_.at[d, q], ssem.at[m], rsem.at[m], dev))
                B.append(remote(s_.at[d, q], b_.at[d, q], ssem.at[m + 1], rsem.at[m + 1], dev))
                C.append(remote(part.at[near_y, 1 - d, q], c_.at[d, q], ssem.at[m + 2], rsem.at[m + 2], dev))
                m += 3
        return C, A, B

    def relay(part, a_, s_, A, B, cuts, k):
        q = slice(*cuts[k])
        for d in range(2):
            n = d * len(cuts) + k
            A[n].wait_recv()
            s_[d, q] = (part[wrap(y + signs[d]), d, q].astype(F32) + a_[d, q].astype(F32)).astype(BF)
            B[n].start()

    cuts = ((0, 80), (80, 128), (128, 160))
    RC, RA, RB = ring(pp, ra, rb, rc, sb, r_s, r_r, cuts)

    halves = (pl.ds(0, D // 2), pl.ds(D // 2, D // 2))

    def spread_first():
        for c in OP:
            c.wait_recv()
        for h in range(2):
            for k in (1, 3, 2):
                for n in range(3):
                    b = wall.at[wrap(y - 1 - n), core, ep, :, halves[h]]
                    remote(b, b, o2_s.at[h, n], o2_r.at[h, n], at_ep(slot(h, k, 0))).start()

    def spread_second():
        for h in range(2):
            for n in range(3):
                rep = wall.at[wrap(y - 1 - n), core, pl.ds(0, 3), :, halves[h]]
                remote(rep, rep, o2_s.at[h, n], o2_r.at[h, n], mate).wait()
        for h in range(2):
            for k in (1, 3, 2):
                for i in range(4):
                    for n in range(3):
                        b = wall.at[wrap(y - 1 - n), core, slot(h, i, 0), :, halves[h]]
                        remote(b, b, o4_s.at[h, n], o4_r.at[h, n], at_ep(slot(h, 0, k))).start()

    def p1_on():
        for h in range(2):
            for d in range(2):
                P1[h, d].wait_recv()
                P1F[h, d].start()
        for h in range(2):
            for i in (1, 2):
                for d in range(2):
                    P2[h, i, d].start()

    def p2_on(i):
        for h in range(2):
            for d in range(2):
                P2[h, i, d].wait_recv()
                P2F[h, i, d].start()

    def p1f_on():
        for h in range(2):
            for d in range(2):
                P1F[h, d].wait_recv()
        for h in range(2):
            for d in range(2):
                P2[h, 3, d].start()

    def near(i, *halves):
        first = halves[0] if halves else 0
        attend_all(2 if halves else 4, lambda n: (first + n // 2, order[i], n % 2 * 2 - 1))

    def far(i):
        for h in range(2):
            for d in range(2):
                P2F[h, i, d].wait_recv()
        attend_all(2, lambda n: (n, order[i], 2))

    for c in locals_:
        c.wait()
    for c in ws:
        c.wait_recv()
    expert([y])
    XA[0][0].wait_recv()
    XR[0].start()
    p1_on()
    p2_on(0)
    spread_first()
    XA[1][1].wait_recv()
    XR[1].start()
    attend_all(8, lambda n: (n // 4, (1 - n // 2 % 2) * (n % 2 * 2 - 1), n // 2 % 2 * (n % 2 * 2 - 1)))
    for d in range(2):
        XC[d].wait_recv()
        XS[d].start()
    XA[0][1].wait_recv()
    XA[1][0].wait_recv()
    expert([wrap(y + 1), wrap(y - 1)])
    def straight(k):
        for d in range(2):
            RC[d * 3 + k].start()

    straight(0)
    p1f_on()
    p2_on(1)
    p2_on(2)
    attend_all(2, lambda n: (n, 2, 0))
    near(1)
    for c in XR + XS:
        c.wait_recv()
    expert([wrap(y + 2)])
    for k in (0, 3, 1, 4, 2, 5):
        RA[k].start()
    near(2)
    p2_on(3)
    spread_second()
    near(3, 0)
    relay(pp, ra, sb, RA, RB, cuts, 0)
    straight(1)
    near(3, 1)
    relay(pp, ra, sb, RA, RB, cuts, 1)
    straight(2)
    far(0)
    relay(pp, ra, sb, RA, RB, cuts, 2)
    far(1)
    far(2)
    far(3)

    for b in range(4):
        for side, dst in ((core, att_loc), (1 - core, att_snd)):
            cols = pl.ds(pl.multiple_of((b * 2 + side) * TOK, TOK), TOK)
            total = jnp.sum(l_s[:, cols], axis=0, keepdims=True)
            dst[b] = (acc[:, cols] / total).astype(BF)
    AT = remote(att_snd, att_rcv, at_s, at_r, mate)
    AT.start()
    AT.wait_recv()
    HD = []
    for b in (1, 3, 2):
        to = wrap(y + b)
        HD.append(remote(att_loc.at[to], hl.at[y], h_s.at[0, b - 1], h_r.at[0, b - 1], at_y(b)))
        HD.append(remote(att_rcv.at[to], hr.at[y], h_s.at[1, b - 1], h_r.at[1, b - 1], at_y(b)))
    for c in HD:
        c.start()
    hl[y] = att_loc[y]
    hr[y] = att_rcv[y]
    def finish(k):
        q = slice(*cuts[k])
        tight = []
        for e in range(2):
            RB[e * 3 + k].wait_recv()
            RC[(1 - e) * 3 + k].wait_recv()
            tight.append((pp[y, e, q].astype(F32) + rb[e, q].astype(F32) + rc[1 - e, q].astype(F32)).astype(BF))
        first, count = ((0, 6), (6, 6), (12, 4))[k]
        for e in range(2):
            rows = tight[e][32:80] if k == 0 else tight[e]
            out[e * 16 + first:e * 16 + first + count] = rows.reshape(count, 8, D)

        def one(n, c):
            g = first + (n + ep) % count
            dst = g * 5 % 16

            @pl.when(dst != ep)
            def _():
                for e in range(2):
                    remote(out.at[e * 16 + g], back.at[e * 16 + ep], m5_s.at[e], m5_r.at[e], at_ep(dst)).start()

            return c

        lax.fori_loop(0, count, one, 0)
        return tight

    compact = jnp.concatenate([t[0:32] for t in finish(0)], 0)
    for n in range(4):
        cols = slice(n * 512, n * 512 + 512)
        wide = lax.dot_general(squeeze, compact[:, cols], tn, preferred_element_type=F32)
        outb[:, :, cols] = wide.reshape(16, 4, 512).astype(BF)

    def last_rows(k, c):
        dst = (ep + k) % 16
        remote(outb.at[dst], backb.at[ep], m5_s.at[2], m5_r.at[2], at_ep(dst)).start()
        return c

    lax.fori_loop(1, 16, last_rows, 0)
    finish(1)
    for n in range(3):
        for h in range(2):
            rep = wall.at[wrap(y - 1 - n), core, pl.ds(0, 12), :, halves[h]]
            remote(rep, rep, o4_s.at[h, n], o4_r.at[h, n], mate).wait()
        WD[n].start()
    finish(2)
    for g in range(2):
        back[g * 16 + ep] = out[g * 16 + place]
    backb[ep] = outb[ep]

    for c in HD + WD:
        c.wait_recv()
    heads = jnp.concatenate([h for b in range(4) for h in (hl[b], hr[b])], 0)
    for q in range(4):
        cols = slice(q * 512, q * 512 + 512)
        w = jnp.concatenate([wall[b, k, :, :, cols].reshape(128, 512) for b in range(4) for k in (core, 1 - core)], 0)
        omix_ref[:, cols] = lax.dot_general(heads, w, tn, preferred_element_type=F32).astype(BF)

    for g in range(2):
        rep = back.at[pl.ds(g * 16, 15)]
        remote(rep, rep, m5_s.at[g], m5_r.at[g], mate).wait()
    rep = backb.at[pl.ds(0, 15)]
    remote(rep, rep, m5_s.at[2], m5_r.at[2], mate).wait()
    rw = rw_ref[...]
    share = rw / jnp.sum(rw, axis=0, keepdims=True)
    w0, w1 = column(share[0:1]), column(share[1:2])
    picks = [
        [jnp.where(c == sid_s[k][:, 0:1], 1.0, 0.0).astype(BF) for c in (slots, slotb)] for k in range(2)
    ]
    for n in range(4):
        cols = slice(n * 512, n * 512 + 512)
        rows = back[:, :, cols].reshape(256, 512)
        more = backb[:, :, cols].reshape(64, 512)
        got = [dot(pick[0], rows) + dot(pick[1], more) for pick in picks]
        oexp_ref[:, cols] = (w0 * got[0] + w1 * got[1]).astype(BF)

    for c in A1 + AL + AR + d1 + ws + XA[0] + XA[1] + XC + XR + XS + RC + RA + RB + OP + WD + HD + [AT]:
        c.wait_send()
    for group in (P1, P1F, P2, P2F):
        for c in group.values():
            c.wait_send()


def tables():
    freq = 1.0 / THETA ** (np.arange(ROPE // 2) * 2.0 / ROPE)
    inner = np.tile(np.arange(TOK)[:, None] * freq, (1, 4))
    first = np.tile(TOK * np.arange(128)[:, None] * freq, (1, 2))
    c, s = np.cos(first), np.sin(first)
    blocks = [[c, s], [-s, c], [s, c], [c, -s]]
    return np.stack(
        [np.cos(inner), np.sin(inner)] + [np.concatenate(b, 1) for b in blocks]
    ).astype(np.float32)


def per_device(
    query_latent, kv_latent, rope_key, query_gain, kv_gain, query_nope_w, query_rope_w,
    key_up_w, value_up_w, output_w, expert_in, moe_gain, routes, route_weight, gate_w, up_w, down_w,
):
    dma = pltpu.SemaphoreType.DMA
    vm = pl.BlockSpec(memory_space=VM)
    hbm = pl.BlockSpec(memory_space=pl.ANY)
    return pl.pallas_call(
        kernel,
        out_shape=(jax.ShapeDtypeStruct((TOK, D), BF), jax.ShapeDtypeStruct((TOK, D), BF)),
        in_specs=[vm] * 14 + [hbm] * 4,
        out_specs=(vm, vm),
        scratch_shapes=[
            VM((8, TOK, LAT), BF), VM((2, 16, KVR, 128), BF), VM((GROUP, 256), BF), VM((GROUP, 256), BF),
            VM((8, GROUP), F32), VM((8, GROUP), F32), VM((VDIM, GROUP), F32),
            VM((4, TOK, 128), BF), VM((4, TOK, 128), BF), VM((4, TOK, 128), BF),
            VM((4, 2, 16, 8, D), BF), VM((4, 128, TOK), BF), VM((4, 128, TOK), BF), VM((2, 2, D, HID), BF), VM((2, 2, D, HID), BF), VM((2, 2, HID, D), BF),
            VM((32, 8, D), BF), VM((16, 4, D), BF), VM((4, 2, 16, 8, D), BF), VM((4, 2, 4, 8, D), BF), VM((16, 4, D), BF), VM((32, 8, D), BF),
            VM((16, 4, D), BF),
            VM((4, 2, 160, D), BF), VM((2, 160, D), BF), VM((2, 160, D), BF), VM((2, 160, D), BF), VM((2, 160, D), BF),
            VM((2, TOK, 128), F32), VM((TOK, D), BF),
            dma((4,)), dma((3,)), dma((3,)), dma((4,)), dma((4,)), dma((6,)), dma((6,)), dma((4,)), dma((4,)),
            dma((2, 4)), dma((2, 4)), dma((2, 4, 4)), dma((2, 4, 4)), dma((2, 3)), dma((2, 3)), dma((2, 2)), dma((2, 2)),
            dma((18,)), dma((18,)), dma((3,)), dma((3,)), dma((2, 3)), dma((2, 3)), dma((2, 3)), dma((2, 3)), dma((3,)), dma((3,)), dma((2, 3)), dma((2, 3)), dma, dma, dma((3,)), dma((3,)),
        ],
        compiler_params=pltpu.CompilerParams(
            collective_id=0, has_side_effects=True, vmem_limit_bytes=66_000_000
        ),
    )(
        query_latent, kv_latent, rope_key.T, query_gain, kv_gain.reshape(1, -1), jnp.asarray(tables()),
        query_nope_w, query_rope_w.T, key_up_w, value_up_w, expert_in, moe_gain.reshape(1, -1), routes.T, route_weight.T,
        output_w.reshape(16, 8, D), gate_w, up_w, down_w,
    )


def solution(mesh):
    rows = P(("ep", "tp"), None)
    placed = (
        rows, rows, rows, P(), P(), P(None, "tp"), P(None, "tp"), P(None, "tp"), P(None, "tp"), P("tp", None),
        rows, P(), rows, rows, P("ep", None, "tp"), P("ep", None, "tp"), P("ep", "tp", None),
    )
    return jax.shard_map(per_device, mesh=mesh, in_specs=placed, out_specs=(rows, rows), check_vma=False)
```

```python
import functools
import math

import jax
import jax.numpy as jnp
import numpy as np
from jax import lax
from jax.experimental import pallas as pl
from jax.experimental.pallas import tpu as pltpu
from jax.sharding import PartitionSpec as P

BF = jnp.bfloat16
F32 = jnp.float32
NOPE, ROPE, VDIM = 128, 64, 128
QLAT, KVLAT, D = 768, 512, 2048
HID = 256
TOK = 128
GROUP = 1024
HALF = 512
LAT = QLAT + KVLAT + 128
KVR = HALF + HALF + HALF // 2
KVH = KVR // 2
QT = 256
THETA = 10000.0
MESH = pl.DeviceIdType.MESH
SCALE2 = math.log2(math.e) / math.sqrt(NOPE + ROPE)
VM = pltpu.VMEM


def dot(a, b):
    return jnp.dot(a, b, preferred_element_type=F32)


def kernel(
    ql_ref, kl_ref, rk_ref, qg_ref, kg_ref, tab_ref, wq_ref, wp_ref, wk_ref, wv_ref,
    xin_ref, mg_ref, routes_ref, rw_ref, ow_hbm, gw_hbm, uw_hbm, dw_hbm,
    both_ref,
    lat, kv, qa, qb, m_s, l_s, acc, att_loc, att_snd, att_rcv,
    wall, hl, hr, gw, uw, dw,
    out, outb, xa, xc, bb, back, backb, pp, ra, rb, rc, sb,
    sid_s, nrm,
    loc_sem, m1_s, m1_r, w_s, w_r, a1_s, a1_r, d1_s, d1_r,
    p1_s, p1_r, p2_s, p2_r, x1_s, x1_r, x2_s, x2_r,
    r_s, r_r, o1_s, o1_r, o2_s, o2_r, o4_s, o4_r, o3_s, o3_r, h_s, h_r, at_s, at_r, m5_s, m5_r,
):
    ep = lax.axis_index("ep")
    tp = lax.axis_index("tp")
    y, core = tp // 2, tp % 2
    z, x = ep // 4, ep % 4
    mate = {"ep": ep, "tp": y * 2 + 1 - core}

    def wrap(a):
        return (a + 4) % 4

    def at_y(dy):
        return {"ep": ep, "tp": wrap(y + dy) * 2 + core}

    def at_ep(e):
        return {"ep": e, "tp": tp}

    def remote(src, dst, ssem, rsem, dev):
        return pltpu.make_async_remote_copy(
            src_ref=src, dst_ref=dst, send_sem=ssem, recv_sem=rsem, device_id=dev, device_id_type=MESH
        )

    barrier = pltpu.get_barrier_semaphore()
    for dy in (1, 2, 3):
        pl.semaphore_signal(barrier, inc=1, device_id=at_y(dy), device_id_type=MESH)
    pl.semaphore_signal(barrier, inc=1, device_id=mate, device_id_type=MESH)

    def greet(k, c):
        pl.semaphore_signal(barrier, inc=1, device_id=at_ep((ep + k) % 16), device_id_type=MESH)
        return c

    lax.fori_loop(1, 16, greet, 0)

    locals_ = [
        pltpu.make_async_copy(gw_hbm, gw.at[0], loc_sem.at[0]),
        pltpu.make_async_copy(uw_hbm, uw.at[0], loc_sem.at[1]),
        pltpu.make_async_copy(dw_hbm, dw.at[0], loc_sem.at[2]),
        pltpu.make_async_copy(ow_hbm, wall.at[y, core], loc_sem.at[3]),
    ]
    for c in locals_:
        c.start()

    f = xin_ref[...].astype(F32)
    cen = f - jnp.mean(f, axis=-1, keepdims=True)
    var = jnp.mean(cen * cen, axis=-1, keepdims=True)
    nrm[...] = (cen * lax.rsqrt(var + 1e-05) * mg_ref[...]).astype(BF)
    rowi = lax.broadcasted_iota(jnp.int32, (TOK, TOK), 0)
    coli = lax.broadcasted_iota(jnp.int32, (TOK, TOK), 1)

    def column(row):
        return jnp.sum(jnp.where(rowi == coli, jnp.broadcast_to(row, (TOK, TOK)), 0.0), axis=1, keepdims=True)

    routes = routes_ref[...].astype(F32)
    r0, r1 = (column(routes[k:k + 1]).astype(jnp.int32) for k in range(2))
    lane = lax.broadcasted_iota(jnp.int32, (TOK, 128), 1)
    oh0 = jnp.where(lane == r0, 1.0, 0.0).astype(F32)
    oh1 = jnp.where(lane == r1, 1.0, 0.0).astype(F32)
    prior = dot(jnp.where(rowi > coli, 1.0, 0.0).astype(BF), (oh0 + oh1).astype(BF))

    def slot_of(r, oh):
        rank = jnp.sum(prior * oh, axis=1, keepdims=True)
        one = (r & 1).astype(F32)
        grp = (r >> 1).astype(F32)
        low = one * 128.0 + grp * 8.0 + rank
        high = 256.0 + grp * 4.0 + one * 2.0 + rank - 8.0
        return jnp.where(rank < 8.0, low, high)

    s0, s1 = slot_of(r0, oh0), slot_of(r1, oh1)
    sid_s[0] = jnp.broadcast_to(s0, (TOK, 128))
    sid_s[1] = jnp.broadcast_to(s1, (TOK, 128))
    slots = lax.broadcasted_iota(jnp.int32, (TOK, 256), 1).astype(F32)
    slotb = lax.broadcasted_iota(jnp.int32, (TOK, 64), 1).astype(F32) + 256.0
    sel = jnp.where((slots == s0) | (slots == s1), 1.0, 0.0).astype(BF)
    selb = jnp.where((slotb == s0) | (slotb == s1), 1.0, 0.0).astype(BF)
    tn = (((0,), (0,)), ((), ()))
    for n in range(4):
        cols = slice(n * 512, n * 512 + 512)
        got = lax.dot_general(sel, nrm[:, cols], tn, preferred_element_type=F32)
        out[:, :, cols] = got.reshape(32, 8, 512).astype(BF)
        got = lax.dot_general(selb, nrm[:, cols], tn, preferred_element_type=F32)
        outb[:, :, cols] = got.reshape(16, 4, 512).astype(BF)

    def rms(ref, gain):
        v = ref[...].astype(F32)
        sq = jnp.mean(v * v, axis=-1, keepdims=True)
        return (v * lax.rsqrt(sq + 1e-06) * gain).astype(BF)

    lat[tp, :, 0:QLAT] = rms(ql_ref, qg_ref[...].reshape(1, QLAT))
    lat[tp, :, QLAT:QLAT + KVLAT] = rms(kl_ref, kg_ref[...])
    i64 = lax.broadcasted_iota(jnp.int32, (ROPE, 128), 0)
    j64 = lax.broadcasted_iota(jnp.int32, (ROPE, 128), 1)
    plain = jnp.where(i64 == j64, 1.0, 0.0) + jnp.where(i64 + 96 == j64, 1.0, 0.0)
    turn = (plain - jnp.where(i64 + 32 == j64, jnp.where(j64 >= 64, 1.0, 0.0), 0.0)).astype(BF)

    def angles(block):
        cb, sb0 = tab_ref[0], tab_ref[1]
        k = [tab_ref[2 + n, pl.ds(block, 1), :] for n in range(4)]
        return cb * k[0] + sb0 * k[1], cb * k[2] + sb0 * k[3]

    def rotated(both, ct, st):
        return (both * ct + pltpu.roll(both, 64, 1) * st).astype(BF)

    lat[tp, :, QLAT + KVLAT:LAT] = rotated(
        lax.dot_general(rk_ref[...], turn, tn, preferred_element_type=F32), *angles(ep * 8 + tp)
    )
    wr = lax.dot_general(wp_ref[...], turn, tn, preferred_element_type=F32).astype(BF)

    pl.semaphore_wait(barrier, 19)

    signs = (1, -1)
    place = ep * 13 % 16

    def m1(e):
        def one(k, c):
            dst = (ep + k) % 16
            if e < 2:
                remote(out.at[e * 16 + dst], xa.at[y, e, place], m1_s.at[e], m1_r.at[e], at_ep(dst)).start()
            else:
                remote(outb.at[dst], bb.at[ep], m1_s.at[2], m1_r.at[2], at_ep(dst)).start()
            return c

        lax.fori_loop(1, 16, one, 0)

    m1(0)
    A1, AL, AR = [], [], []
    rowsof = (pl.ds(0, 64), pl.ds(64, 64))
    for d in range(2):
        first, last = lat.at[tp, rowsof[d]], lat.at[tp, rowsof[1 - d]]
        A1.append(remote(first, first, a1_s.at[d], a1_r.at[d], at_y(signs[d])))
        AL.append(remote(last, last, a1_s.at[2 + d], a1_r.at[2 + d], at_y(signs[d])))
        fw = lat.at[wrap(y - signs[d]) * 2 + core, rowsof[d]]
        AR.append(remote(fw, fw, a1_s.at[4 + d], a1_r.at[4 + d], at_y(signs[d])))
    for c in A1 + AL:
        c.start()
    m1(1)
    m1(2)
    d1 = []
    for dy in (0, 1, 3, 2):
        t = wrap(y - dy) * 2 + core
        d1.append(remote(lat.at[t], lat.at[t], d1_s.at[dy], d1_r.at[dy], mate))
    d1[0].start()
    ws = [
        remote(gw_hbm, gw.at[1], w_s.at[0], w_r.at[0], mate),
        remote(uw_hbm, uw.at[1], w_s.at[1], w_r.at[1], mate),
        remote(dw_hbm, dw.at[1], w_s.at[2], w_r.at[2], mate),
        remote(ow_hbm, wall.at[y, core], w_s.at[3], w_r.at[3], mate),
    ]
    for c in ws:
        c.start()
    OP, WD = [], []
    for dy in range(1, 4):
        OP.append(remote(ow_hbm.at[ep], wall.at[y, core, ep], o1_s.at[dy - 1], o1_r.at[dy - 1], at_y(dy)))
        b = wall.at[wrap(y - dy), core]
        WD.append(remote(b, b, o3_s.at[dy - 1], o3_r.at[dy - 1], mate))
    for c in OP:
        c.start()

    for e in range(2):
        xa[y, e, place] = out[e * 16 + ep]
    bb[ep] = outb[ep]

    XA, XC, XR, XS = [], [], [], []
    for d in range(2):
        dev = at_y(signs[d])
        XA.append([remote(xa.at[y, e], xa.at[y, e], x1_s.at[d, e], x1_r.at[d, e], dev) for e in range(2)])
        XC.append(remote(xc.at[y], xc.at[y], x1_s.at[d, 2], x1_r.at[d, 2], dev))
        b = wrap(y - signs[d])
        XR.append(remote(xa.at[b, d], xa.at[b, d], x2_s.at[d, 0], x2_r.at[d, 0], dev))
        XS.append(remote(xc.at[b, d], xc.at[b, d], x2_s.at[d, 1], x2_r.at[d, 1], dev))

    def rows_here(e):
        rep = xa.at[y, e, pl.ds(0, 15)]
        remote(rep, rep, m1_s.at[e], m1_r.at[e], mate).wait()
        for d in range(2):
            XA[d][e].start()

    for d in range(2):
        A1[d].wait_recv()
        AR[d].start()
    rows_here(0)
    for d in range(2):
        AL[d].wait_recv()
        d1[1 + d].start()
    for c in AR:
        c.wait_recv()
    d1[3].start()
    rows_here(1)
    rep = bb.at[pl.ds(0, 15)]
    remote(rep, rep, m1_s.at[2], m1_r.at[2], mate).wait()
    row64 = lax.broadcasted_iota(jnp.int32, (64, 64), 0)
    col64 = lax.broadcasted_iota(jnp.int32, (64, 64), 1)
    want = ((row64 & 31) >> 1) * 4 + (row64 >> 5) * 2 + (row64 & 1)
    squeeze = jnp.where(want == col64, 1.0, 0.0).astype(BF)
    for n in range(4):
        cols = slice(n * 512, n * 512 + 512)
        tight = dot(squeeze, bb[:, :, cols].reshape(64, 512))
        xc[y, :, :, :, cols] = tight.reshape(2, 4, 8, 512).astype(BF)
    for c in XC:
        c.start()
    for c in d1:
        c.wait_recv()

    lane128 = lax.broadcasted_iota(jnp.int32, (HALF // 2, 128), 1)
    lane512 = lax.broadcasted_iota(jnp.int32, (HALF, 128), 1)
    for h in range(2):
        part = lat[h * 4:h * 4 + 4]
        qn = part[:, :, 0:QLAT].reshape(HALF, QLAT)
        kvn = part[:, :, QLAT:QLAT + KVLAT].reshape(HALF, KVLAT)
        rows = slice(h * HALF, h * HALF + HALF)
        qf = dot(qn, wq_ref[...])
        tabs = [angles(ep * 8 + h * 4 + t) for t in range(4)]
        rot = rotated(
            dot(qn, wr), jnp.concatenate([t[0] for t in tabs], 0), jnp.concatenate([t[1] for t in tabs], 0)
        )
        zero = jnp.zeros_like(rot)
        qa[rows, 0:128] = qf.astype(BF)
        qb[rows, 0:128] = qf.astype(BF)
        qa[rows, 128:256] = jnp.where(lane512 < 64, rot, zero)
        qb[rows, 128:256] = jnp.where(lane512 < 64, zero, rot)
        kv[h, ep, 0:HALF] = dot(kvn, wk_ref[...]).astype(BF)
        turned = jnp.transpose(dot(kvn, wv_ref[...])).astype(BF)
        for t in range(4):
            kv[h, ep, HALF + t * 128:HALF + t * 128 + 128] = turned[:, t * 128:t * 128 + 128]
        lo = part[0:2, :, QLAT + KVLAT:LAT].reshape(HALF // 2, 128)
        hi = part[2:4, :, QLAT + KVLAT:LAT].reshape(HALF // 2, 128)
        kv[h, ep, 2 * HALF:KVR] = jnp.where(lane128 < 64, lo, hi)

    def slot(h, du, dv):
        if h == 0:
            return wrap(z + dv) * 4 + wrap(x + du)
        return wrap(z + du) * 4 + wrap(x + dv)

    pieces = (slice(0, KVH), slice(KVH, KVR))
    order = (0, -1, 1, 2)
    P1, P1F, P2, P2F = {}, {}, {}, {}
    for h in range(2):
        for d in range(2):
            sg = signs[d]
            own = kv.at[h, slot(h, 0, 0)]
            P1[h, d] = remote(own, own, p1_s.at[h, d], p1_r.at[h, d], at_ep(slot(h, sg, 0)))
            fw = kv.at[h, slot(h, -sg, 0), pieces[d]]
            P1F[h, d] = remote(fw, fw, p1_s.at[h, 2 + d], p1_r.at[h, 2 + d], at_ep(slot(h, sg, 0)))
            for i in range(4):
                own = kv.at[h, slot(h, order[i], 0)]
                P2[h, i, d] = remote(own, own, p2_s.at[h, i, d], p2_r.at[h, i, d], at_ep(slot(h, 0, sg)))
                fw = kv.at[h, slot(h, order[i], -sg), pieces[d]]
                P2F[h, i, d] = remote(fw, fw, p2_s.at[h, i, 2 + d], p2_r.at[h, i, 2 + d], at_ep(slot(h, 0, sg)))

    for h in range(2):
        for d in range(2):
            P1[h, d].start()

    nt = (((1,), (1,)), ((), ()))

    def tile(qi):
        return pl.ds(qi * QT, QT)

    def scores(h, src, qi, masked):
        rots = kv[h, src, 2 * HALF:KVR]
        low = jnp.concatenate([kv[h, src, 0:256], rots], 1)
        high = jnp.concatenate([kv[h, src, 256:512], rots], 1)
        s = jnp.concatenate(
            [
                lax.dot_general(low, qa[tile(qi)], nt, preferred_element_type=F32),
                lax.dot_general(high, qb[tile(qi)], nt, preferred_element_type=F32),
            ],
            0,
        )
        if masked:
            kp = h * HALF + lax.broadcasted_iota(jnp.int32, (HALF, QT), 0)
            qp = qi * QT + lax.broadcasted_iota(jnp.int32, (HALF, QT), 1)
            s = jnp.where(kp <= qp, s, -1e30)
        return s

    def weigh(s, qi):
        old = m_s[:, tile(qi)]
        new = jnp.maximum(old, jnp.max(s, axis=0, keepdims=True))
        p = jnp.exp2((s - new[0:1]) * SCALE2)
        fac = jnp.exp2((old - new) * SCALE2)
        m_s[:, tile(qi)] = new
        l_s[:, tile(qi)] = l_s[:, tile(qi)] * fac + jnp.sum(p.reshape(HALF // 8, 8, QT), axis=0)
        return p.astype(BF), fac

    def gather_values(p, fac, h, src, qi):
        vals = jnp.concatenate([kv[h, src, HALF + t * 128:HALF + t * 128 + 128] for t in range(4)], 1)
        acc[:, tile(qi)] = acc[:, tile(qi)] * fac[0:1] + dot(vals, p)

    def run(items):
        s, prev = scores(*items[0]), None
        for n, (h, src, qi, _) in enumerate(items):
            later = scores(*items[n + 1]) if n + 1 < len(items) else None
            weighed = weigh(s, qi)
            if prev is not None:
                gather_values(*prev)
            prev, s = weighed + (h, src, qi), later
        gather_values(*prev)

    def attend_all(count, place):
        def one(n, c):
            h, du, dv = place(n)
            src = wrap(z + dv + h * (du - dv)) * 4 + wrap(x + du + h * (dv - du))

            @pl.when(src < ep)
            def _():
                run([(h, src, qi, False) for qi in range(GROUP // QT)])

            return c

        lax.fori_loop(0, count, one, 0)

    m_s[...] = jnp.full((8, GROUP), -1e30, F32)
    l_s[...] = jnp.zeros((8, GROUP), F32)
    acc[...] = jnp.zeros((VDIM, GROUP), F32)
    run([(0, ep, 0, True), (0, ep, 1, True), (0, ep, 2, False), (0, ep, 3, False), (1, ep, 2, True), (1, ep, 3, True)])

    for h in range(2):
        for d in range(2):
            P2[h, 0, d].start()

    def expert(ys):
        n = len(ys)

        def one(e, c):
            rows = jnp.concatenate([r for b in ys for r in (xc[b, e].reshape(32, D), xa[b, e].reshape(128, D))], 0)
            total = [None] * 4
            hid = []
            for w in range(2):
                g = jnp.minimum(dot(rows, gw[w, e]), 7.0)
                u = jnp.clip(dot(rows, uw[w, e]), -7.0, 7.0)
                hid.append((g * jax.nn.sigmoid(1.702 * g) * (u + 1.0)).astype(BF))
            both = jnp.concatenate(hid, 1)
            for q in range(4):
                cols = slice(q * 512, q * 512 + 512)
                down = jnp.concatenate([dw[0, e, :, cols], dw[1, e, :, cols]], 0)
                total = dot(both, down).astype(BF)
                for k in range(n):
                    pp[ys[k], e, :, cols] = total[k * 160:k * 160 + 160]
            return c

        lax.fori_loop(0, 2, one, 0)

    def ring(part, a_, b_, c_, s_, ssem, rsem, cuts):
        C, A, B = [], [], []
        m = 0
        for d in range(2):
            dev = at_y(signs[d])
            near_y = wrap(y + signs[d])
            for lo, hi in cuts:
                q = pl.ds(lo, hi - lo)
                A.append(remote(part.at[wrap(y + 2), d, q], a_.at[d, q], ssem.at[m], rsem.at[m], dev))
                B.append(remote(s_.at[d, q], b_.at[d, q], ssem.at[m + 1], rsem.at[m + 1], dev))
                C.append(remote(part.at[near_y, 1 - d, q], c_.at[d, q], ssem.at[m + 2], rsem.at[m + 2], dev))
                m += 3
        return C, A, B

    def relay(part, a_, s_, A, B, cuts, k):
        q = slice(*cuts[k])
        for d in range(2):
            n = d * len(cuts) + k
            A[n].wait_recv()
            s_[d, q] = (part[wrap(y + signs[d]), d, q].astype(F32) + a_[d, q].astype(F32)).astype(BF)
            B[n].start()

    cuts = ((0, 80), (80, 128), (128, 160))
    RC, RA, RB = ring(pp, ra, rb, rc, sb, r_s, r_r, cuts)

    halves = (pl.ds(0, D // 2), pl.ds(D // 2, D // 2))

    def spread_first():
        for c in OP:
            c.wait_recv()
        for h in range(2):
            for k in (1, 3, 2):
                for n in range(3):
                    b = wall.at[wrap(y - 1 - n), core, ep, :, halves[h]]
                    remote(b, b, o2_s.at[h, n], o2_r.at[h, n], at_ep(slot(h, k, 0))).start()

    def spread_second():
        for h in range(2):
            for n in range(3):
                rep = wall.at[wrap(y - 1 - n), core, pl.ds(0, 3), :, halves[h]]
                remote(rep, rep, o2_s.at[h, n], o2_r.at[h, n], mate).wait()
        for h in range(2):
            for k in (1, 3, 2):
                for i in range(4):
                    for n in range(3):
                        b = wall.at[wrap(y - 1 - n), core, slot(h, i, 0), :, halves[h]]
                        remote(b, b, o4_s.at[h, n], o4_r.at[h, n], at_ep(slot(h, 0, k))).start()

    def p1_on():
        for h in range(2):
            for d in range(2):
                P1[h, d].wait_recv()
                P1F[h, d].start()
        for h in range(2):
            for i in (1, 2):
                for d in range(2):
                    P2[h, i, d].start()

    def p2_on(i):
        for h in range(2):
            for d in range(2):
                P2[h, i, d].wait_recv()
                P2F[h, i, d].start()

    def p1f_on():
        for h in range(2):
            for d in range(2):
                P1F[h, d].wait_recv()
        for h in range(2):
            for d in range(2):
                P2[h, 3, d].start()

    def near(i, *halves):
        first = halves[0] if halves else 0
        attend_all(2 if halves else 4, lambda n: (first + n // 2, order[i], n % 2 * 2 - 1))

    def far(i):
        for h in range(2):
            for d in range(2):
                P2F[h, i, d].wait_recv()
        attend_all(2, lambda n: (n, order[i], 2))

    for c in locals_:
        c.wait()
    for c in ws:
        c.wait_recv()
    expert([y])
    XA[0][0].wait_recv()
    XR[0].start()
    p1_on()
    p2_on(0)
    spread_first()
    XA[1][1].wait_recv()
    XR[1].start()
    attend_all(8, lambda n: (n // 4, (1 - n // 2 % 2) * (n % 2 * 2 - 1), n // 2 % 2 * (n % 2 * 2 - 1)))
    for d in range(2):
        XC[d].wait_recv()
        XS[d].start()
    XA[0][1].wait_recv()
    XA[1][0].wait_recv()
    expert([wrap(y + 1), wrap(y - 1)])
    def straight(k):
        for d in range(2):
            RC[d * 3 + k].start()

    straight(0)
    p1f_on()
    p2_on(1)
    p2_on(2)
    attend_all(2, lambda n: (n, 2, 0))
    near(1)
    for c in XR + XS:
        c.wait_recv()
    expert([wrap(y + 2)])
    for k in (0, 3, 1, 4, 2, 5):
        RA[k].start()
    near(2)
    p2_on(3)
    spread_second()
    near(3, 0)
    relay(pp, ra, sb, RA, RB, cuts, 0)
    straight(1)
    near(3, 1)
    relay(pp, ra, sb, RA, RB, cuts, 1)
    straight(2)
    far(0)
    relay(pp, ra, sb, RA, RB, cuts, 2)
    far(1)
    far(2)
    far(3)

    for b in range(4):
        for side, dst in ((core, att_loc), (1 - core, att_snd)):
            cols = pl.ds(pl.multiple_of((b * 2 + side) * TOK, TOK), TOK)
            total = jnp.sum(l_s[:, cols], axis=0, keepdims=True)
            dst[b] = (acc[:, cols] / total).astype(BF)
    AT = remote(att_snd, att_rcv, at_s, at_r, mate)
    AT.start()
    AT.wait_recv()
    HD = []
    for b in (1, 3, 2):
        to = wrap(y + b)
        HD.append(remote(att_loc.at[to], hl.at[y], h_s.at[0, b - 1], h_r.at[0, b - 1], at_y(b)))
        HD.append(remote(att_rcv.at[to], hr.at[y], h_s.at[1, b - 1], h_r.at[1, b - 1], at_y(b)))
    for c in HD:
        c.start()
    hl[y] = att_loc[y]
    hr[y] = att_rcv[y]
    def finish(k):
        q = slice(*cuts[k])
        tight = []
        for e in range(2):
            RB[e * 3 + k].wait_recv()
            RC[(1 - e) * 3 + k].wait_recv()
            tight.append((pp[y, e, q].astype(F32) + rb[e, q].astype(F32) + rc[1 - e, q].astype(F32)).astype(BF))
        first, count = ((0, 6), (6, 6), (12, 4))[k]
        for e in range(2):
            rows = tight[e][32:80] if k == 0 else tight[e]
            out[e * 16 + first:e * 16 + first + count] = rows.reshape(count, 8, D)

        def one(n, c):
            g = first + (n + ep) % count
            dst = g * 5 % 16

            @pl.when(dst != ep)
            def _():
                for e in range(2):
                    remote(out.at[e * 16 + g], back.at[e * 16 + ep], m5_s.at[e], m5_r.at[e], at_ep(dst)).start()

            return c

        lax.fori_loop(0, count, one, 0)
        return tight

    compact = jnp.concatenate([t[0:32] for t in finish(0)], 0)
    for n in range(4):
        cols = slice(n * 512, n * 512 + 512)
        wide = lax.dot_general(squeeze, compact[:, cols], tn, preferred_element_type=F32)
        outb[:, :, cols] = wide.reshape(16, 4, 512).astype(BF)

    def last_rows(k, c):
        dst = (ep + k) % 16
        remote(outb.at[dst], backb.at[ep], m5_s.at[2], m5_r.at[2], at_ep(dst)).start()
        return c

    lax.fori_loop(1, 16, last_rows, 0)
    finish(1)
    for n in range(3):
        for h in range(2):
            rep = wall.at[wrap(y - 1 - n), core, pl.ds(0, 12), :, halves[h]]
            remote(rep, rep, o4_s.at[h, n], o4_r.at[h, n], mate).wait()
        WD[n].start()
    finish(2)
    for g in range(2):
        back[g * 16 + ep] = out[g * 16 + place]
    backb[ep] = outb[ep]

    for c in HD + WD:
        c.wait_recv()
    heads = jnp.concatenate([h for b in range(4) for h in (hl[b], hr[b])], 0)
    for q in range(4):
        cols = slice(q * 512, q * 512 + 512)
        w = jnp.concatenate([wall[b, k, :, :, cols].reshape(128, 512) for b in range(4) for k in (core, 1 - core)], 0)
        both_ref[0, :, cols] = lax.dot_general(heads, w, tn, preferred_element_type=F32).astype(BF)

    for g in range(2):
        rep = back.at[pl.ds(g * 16, 15)]
        remote(rep, rep, m5_s.at[g], m5_r.at[g], mate).wait()
    rep = backb.at[pl.ds(0, 15)]
    remote(rep, rep, m5_s.at[2], m5_r.at[2], mate).wait()
    rw = rw_ref[...]
    share = rw / jnp.sum(rw, axis=0, keepdims=True)
    w0, w1 = column(share[0:1]), column(share[1:2])
    picks = [
        [jnp.where(c == sid_s[k][:, 0:1], 1.0, 0.0).astype(BF) for c in (slots, slotb)] for k in range(2)
    ]
    for n in range(4):
        cols = slice(n * 512, n * 512 + 512)
        rows = back[:, :, cols].reshape(256, 512)
        more = backb[:, :, cols].reshape(64, 512)
        got = [dot(pick[0], rows) + dot(pick[1], more) for pick in picks]
        both_ref[1, :, cols] = (w0 * got[0] + w1 * got[1]).astype(BF)

    for c in A1 + AL + AR + d1 + ws + XA[0] + XA[1] + XC + XR + XS + RC + RA + RB + OP + WD + HD + [AT]:
        c.wait_send()
    for group in (P1, P1F, P2, P2F):
        for c in group.values():
            c.wait_send()


def tables():
    freq = 1.0 / THETA ** (np.arange(ROPE // 2) * 2.0 / ROPE)
    inner = np.tile(np.arange(TOK)[:, None] * freq, (1, 4))
    first = np.tile(TOK * np.arange(128)[:, None] * freq, (1, 2))
    c, s = np.cos(first), np.sin(first)
    blocks = [[c, s], [-s, c], [s, c], [c, -s]]
    return np.stack(
        [np.cos(inner), np.sin(inner)] + [np.concatenate(b, 1) for b in blocks]
    ).astype(np.float32)


def per_device(
    query_latent, kv_latent, rope_key, query_gain, kv_gain, query_nope_w, query_rope_w,
    key_up_w, value_up_w, output_w, expert_in, moe_gain, routes, route_weight, gate_w, up_w, down_w,
):
    dma = pltpu.SemaphoreType.DMA
    vm = pl.BlockSpec(memory_space=VM)
    hbm = pl.BlockSpec(memory_space=pl.ANY)
    both = pl.pallas_call(
        kernel,
        out_shape=jax.ShapeDtypeStruct((2, TOK, D), BF),
        in_specs=[vm] * 14 + [hbm] * 4,
        out_specs=vm,
        scratch_shapes=[
            VM((8, TOK, LAT), BF), VM((2, 16, KVR, 128), BF), VM((GROUP, 256), BF), VM((GROUP, 256), BF),
            VM((8, GROUP), F32), VM((8, GROUP), F32), VM((VDIM, GROUP), F32),
            VM((4, TOK, 128), BF), VM((4, TOK, 128), BF), VM((4, TOK, 128), BF),
            VM((4, 2, 16, 8, D), BF), VM((4, 128, TOK), BF), VM((4, 128, TOK), BF), VM((2, 2, D, HID), BF), VM((2, 2, D, HID), BF), VM((2, 2, HID, D), BF),
            VM((32, 8, D), BF), VM((16, 4, D), BF), VM((4, 2, 16, 8, D), BF), VM((4, 2, 4, 8, D), BF), VM((16, 4, D), BF), VM((32, 8, D), BF),
            VM((16, 4, D), BF),
            VM((4, 2, 160, D), BF), VM((2, 160, D), BF), VM((2, 160, D), BF), VM((2, 160, D), BF), VM((2, 160, D), BF),
            VM((2, TOK, 128), F32), VM((TOK, D), BF),
            dma((4,)), dma((3,)), dma((3,)), dma((4,)), dma((4,)), dma((6,)), dma((6,)), dma((4,)), dma((4,)),
            dma((2, 4)), dma((2, 4)), dma((2, 4, 4)), dma((2, 4, 4)), dma((2, 3)), dma((2, 3)), dma((2, 2)), dma((2, 2)),
            dma((18,)), dma((18,)), dma((3,)), dma((3,)), dma((2, 3)), dma((2, 3)), dma((2, 3)), dma((2, 3)), dma((3,)), dma((3,)), dma((2, 3)), dma((2, 3)), dma, dma, dma((3,)), dma((3,)),
        ],
        compiler_params=pltpu.CompilerParams(
            collective_id=0, has_side_effects=True, vmem_limit_bytes=66_000_000
        ),
    )(
        query_latent, kv_latent, rope_key.T, query_gain, kv_gain.reshape(1, -1), jnp.asarray(tables()),
        query_nope_w, query_rope_w.T, key_up_w, value_up_w, expert_in, moe_gain.reshape(1, -1), routes.T, route_weight.T,
        output_w.reshape(16, 8, D), gate_w, up_w, down_w,
    )
    return both[0], both[1]


def solution(mesh):
    rows = P(("ep", "tp"), None)
    placed = (
        rows, rows, rows, P(), P(), P(None, "tp"), P(None, "tp"), P(None, "tp"), P(None, "tp"), P("tp", None),
        rows, P(), rows, rows, P("ep", None, "tp"), P("ep", None, "tp"), P("ep", "tp", None),
    )
    return jax.shard_map(per_device, mesh=mesh, in_specs=placed, out_specs=(rows, rows), check_vma=False)
```
